32 devices in a mesh: grp: 2 (over x), ep: 16 (over z, y, core).
Axes of the slice: x: 2, y: 2, z: 4, core: 2. Of those that a mesh axis runs over, the one named last changes fastest.
Arguments:
- tokens: bfloat16 [128, 2048], P(('grp', 'ep')), parts along dimension 0, may hold values from -30 to 30
- state: float32 [128, 16, 128, 128], P(('grp', 'ep')), parts along dimension 0, may hold values from -6 to 6
- route_ids: int32 [128, 2], P(('grp', 'ep')), parts along dimension 0, may hold values from 0 to 3, all different within a row; in each aligned block of 4 rows (0 to 3, 4 to 7, ...) at most 3 rows name the same one
- route_weights: bfloat16 [128, 2], P(('grp', 'ep')), parts along dimension 0, may hold values from 0.099609375 to 1
- norm_mix: float32 [2048], replicated, may hold values from 0.1 to 1.9
- w_query: bfloat16 [2048, 2048], P(None, 'ep'), may hold values from -0.125 to 0.125
- w_forget: bfloat16 [2048, 2048], P(None, 'ep'), may hold values from -0.125 to 0.125
- w_input: bfloat16 [2048, 2048], P(None, 'ep'), may hold values from -0.125 to 0.125
- w_gate: bfloat16 [2048, 2048], P(None, 'ep'), may hold values from -0.125 to 0.125
- lower_bound: float32 [2048], replicated, may hold values from 0.05 to 0.9
- head_gain: float32 [128], replicated, may hold values from 0.1 to 1.9
- w_out: bfloat16 [2048, 2048], P(None, 'ep'), may hold values from -0.125 to 0.125
- norm_ffn: float32 [2048], replicated, may hold values from 0.1 to 1.9
- expert_gate: bfloat16 [2048, 28672], P(None, 'ep'), may hold values from -0.125 to 0.125
- expert_up: bfloat16 [2048, 28672], P(None, 'ep'), may hold values from -0.125 to 0.125
- expert_down: bfloat16 [28672, 2048], P('ep'), may hold values from -0.0625 to 0.0625
Outputs:
- layer_out: bfloat16 [128, 2048], P(('grp', 'ep')), parts along dimension 0
- new_state: float32 [128, 16, 128, 128], P(('grp', 'ep')), parts along dimension 0
The draws below stay inside these ranges and needn't reach their ends.
There are 2 independent parts, one for each index of `grp`. The reference program is written for one: setup_inputs(seed, part) draws one part's arguments, and reference() takes and returns one part's arrays. A program takes and returns all parts, laid end to end along the dimension named above; an argument that names none is the same for every part. Nothing has to cross between parts.
Inputs may be any that keep to these rules, and one draw needn't show every extreme that they name: `route_ids`: each row names 2 different experts; the rows of one device name no expert more than 3 times, and some device names one exactly 3 times.
All inputs are finite; a program needn't handle non-finite values.
Results may differ from the reference program's by a relative error of at most 0.008.
Values may be sent and summed in bfloat16 or wider, within the bound.
A program may use at most 64 MiB of HBM per device.

```python
import math
import jax
import jax.numpy as jnp
import numpy as np
from jax import lax

D = 2048
HEAD_DIM = 128
HEADS = 16
FF = 7168
EXPERTS = 4
TOP_K = 2
SEQ_DEV = 4
TOKENS = 64
CAP = 3


def draw_tokens(key, part):
    row_key, col_key, value_key = jax.random.split(key, 3)
    col_scale = jnp.exp(jnp.linspace(jnp.log(0.3), jnp.log(3.0), D))
    col_scale = col_scale * jnp.exp(jax.random.uniform(col_key, (D,), jnp.float32, -0.35, 0.35))
    row_scale = jnp.exp(jax.random.uniform(row_key, (TOKENS, 1), jnp.float32, jnp.log(0.5), jnp.log(1.5)))
    values = jax.random.normal(value_key, (TOKENS, D), jnp.float32)
    return jnp.clip(values * row_scale * col_scale[None, :], -30.0, 30.0).astype(jnp.bfloat16)


def block_scale(own_key, shape, cuts, low, top_value):
    factor_of, own = 1.0, jax.random.fold_in(own_key, 6)
    for position, shards_of in cuts:
        steps = jnp.exp(jax.random.uniform(jax.random.fold_in(own, position), (shards_of,), jnp.float32, low / len(cuts), top_value / len(cuts)))
        factor_of = factor_of * jnp.repeat(steps, shape[position] // shards_of).reshape([-1 if axis == position else 1 for axis in range(len(shape))])
    return factor_of


def assign_block(rng, own, number, rows, count, top, most, skew):
    ranking = jax.random.permutation(rng, count)
    heavy_load, ordinary = load_shares(count, rows * top, most, skew, True), load_shares(count, rows * top, most, skew, False)
    places = jnp.arange(count)

    def named(tallies, offset_by):
        used = int((tallies > 0).sum())
        fixed = max(1, used // 4)
        shifted = fixed + (places - fixed + offset_by * (used - fixed)) % max(1, count - fixed)
        return jnp.zeros((count,), jnp.int32).at[ranking[jnp.where(places < fixed, places, shifted)]].set(jnp.asarray(tallies, jnp.int32))

    tallies = jnp.where(number % 4 == 0, named(heavy_load, number // 4), named(ordinary, number - number // 4 - 1))
    mixed = jax.random.permutation(jax.random.fold_in(own, 3), count)
    giver, receiver = mixed[0:count // 2 * 2:2], mixed[1:count // 2 * 2:2]
    slack = jnp.minimum(tallies[giver] - 1, most - tallies[receiver]) // 2
    slack = jnp.where((giver == ranking[0]) | (receiver == ranking[0]) | (tallies[receiver] == 0), 0, jnp.maximum(slack, 0))
    shifted = jax.random.randint(jax.random.fold_in(own, 4), (count // 2,), 0, 1 << 20) % (slack + 1)
    tallies = tallies.at[giver].add(-shifted).at[receiver].add(shifted)
    members = jnp.searchsorted(jnp.cumsum(tallies), jnp.arange(rows * top), side="right").astype(jnp.int32)
    grid = members.reshape(top, rows).T
    grid = grid[jax.random.permutation(jax.random.fold_in(own, 1), rows)]
    offset_by = jax.random.randint(jax.random.fold_in(own, 2), (rows, 1), 0, top)
    return jnp.take_along_axis(grid, (jnp.arange(top)[None, :] + offset_by) % top, axis=1)


def load_shares(amount, total, limit, lean, full):
    weights = [(1 << 20) // math.isqrt(rank ** lean) + 1 for rank in range(1, amount + 1)]
    largest = limit if full else min(limit, max(-(-total // amount), total * weights[0] // sum(weights)))
    least = 1 if total - largest >= amount - 1 else 0
    given, spare = [largest] + [least] * (amount - 1), total - largest - least * (amount - 1)
    while spare > 0:
        movable = [i for i in range(1, amount) if given[i] < largest] or [i for i in range(1, amount) if given[i] < limit]
        pool, left = sum([weights[i] for i in movable]), spare
        for i in movable:
            extra = min(limit - given[i], max(1, left * weights[i] // pool), spare)
            given[i] = given[i] + extra
            spare = spare - extra
    return np.array(given)


def centred(own_key, dims, spread, bound, pieces=(), held_as=jnp.bfloat16):
    factor_of = block_scale(own_key, dims, pieces, -0.22, 0.18) if pieces else 1.0
    result = jax.random.normal(own_key, dims, jnp.float32) * spread * factor_of
    return jnp.minimum(jnp.maximum(result, -bound), bound).astype(held_as)


def setup_inputs(seed: int = 0, part: int = 0) -> dict:
    splits = jax.random.split(jax.random.key(seed), 17)
    part_keys = jax.random.split(jax.random.fold_in(splits[16], part), 17)
    tokens = draw_tokens(jax.random.fold_in(jax.random.fold_in(splits[16], part), 71), part)
    state = centred(part_keys[1], (TOKENS, HEADS, HEAD_DIM, HEAD_DIM), 1.0, 6.0, ((0, 16),), jnp.float32)
    route_ids_keys = jax.random.split(jax.random.fold_in(part_keys[2], 1), TOKENS // SEQ_DEV)
    route_ids_turns = jax.random.permutation(jax.random.fold_in(part_keys[2], 3), TOKENS // SEQ_DEV)
    route_ids = jax.vmap(lambda own, number: assign_block(jax.random.fold_in(part_keys[2], 2), own, number, SEQ_DEV, EXPERTS, TOP_K, CAP, 1))(route_ids_keys, route_ids_turns).reshape((TOKENS, TOP_K))
    route_weights = jnp.clip(0.099609375 + 0.9003906 * jax.random.uniform(part_keys[3], (TOKENS, TOP_K), jnp.float32) ** block_scale(part_keys[3], (TOKENS, TOP_K), ((0, 16),), -0.2, 0.2), 0.099609375, 1.0).astype(jnp.bfloat16)
    norm_mix = jnp.clip(1.0 + 0.18 * jax.random.normal(splits[4], (D,), jnp.float32), 0.1, 1.9)
    w_query = centred(splits[5], (D, D), D ** -0.5, 0.125, ((1, 16),))
    w_forget = centred(splits[6], (D, D), D ** -0.5, 0.125, ((1, 16),))
    w_input = centred(splits[7], (D, D), D ** -0.5, 0.125, ((1, 16),))
    w_gate = centred(splits[8], (D, D), D ** -0.5, 0.125, ((1, 16),))
    lower_bound = jnp.clip(jax.random.uniform(splits[9], (D,), jnp.float32, 0.05, 0.9), 0.05, 0.9)
    head_gain = jnp.clip(1.0 + 0.18 * jax.random.normal(splits[10], (HEAD_DIM,), jnp.float32), 0.1, 1.9)
    w_out = centred(splits[11], (D, D), D ** -0.5, 0.125, ((1, 16),))
    norm_ffn = jnp.clip(1.0 + 0.18 * jax.random.normal(splits[12], (D,), jnp.float32), 0.1, 1.9)
    expert_gate = centred(splits[13], (D, EXPERTS * FF), D ** -0.5, 0.125, ((1, 16),))
    expert_up = centred(splits[14], (D, EXPERTS * FF), D ** -0.5, 0.125, ((1, 16),))
    expert_down = centred(splits[15], (EXPERTS * FF, D), FF ** -0.5, 0.0625, ((0, 16),))
    return dict(tokens=tokens, state=state, route_ids=route_ids, route_weights=route_weights, norm_mix=norm_mix, w_query=w_query, w_forget=w_forget, w_input=w_input, w_gate=w_gate, lower_bound=lower_bound, head_gain=head_gain, w_out=w_out, norm_ffn=norm_ffn, expert_gate=expert_gate, expert_up=expert_up, expert_down=expert_down)


epsilon = 1e-06

def rms_scale(values, gain):
    return values * lax.rsqrt(lax.optimization_barrier(jnp.mean(values * values, axis=-1, keepdims=True)) + epsilon) * gain

def mixer_state(projected, state, lower_bound, head_gain):
    query_raw = projected[0].astype(jnp.float32)
    forget_raw = projected[1].astype(jnp.float32)
    input_raw = projected[2].astype(jnp.float32)
    gate_raw = projected[3].astype(jnp.float32)
    seq_rows = state.shape[0]
    heads = state.shape[1]
    head_dim = state.shape[2]
    head_shape = (seq_rows, heads, head_dim)
    floor_rate = lower_bound.astype(jnp.float32)
    log_forget = jnp.logaddexp(jnp.log(floor_rate), jnp.log1p(-floor_rate) + jax.nn.log_sigmoid(forget_raw))
    key_vec = (1.0 - floor_rate) * jax.nn.sigmoid(-forget_raw)
    query_vec = jax.nn.silu(query_raw) * head_dim ** (-0.5)
    new_state = jnp.exp(log_forget).reshape(head_shape)[..., None] * state + key_vec.reshape(head_shape)[..., None] * input_raw.reshape(head_shape)[:, :, None, :]
    read_out = jnp.einsum('thk,thkv->thv', query_vec.reshape(head_shape), new_state, precision=lax.Precision.HIGHEST)
    mixed = rms_scale(read_out, head_gain) * jax.nn.silu(gate_raw.reshape(head_shape))
    return (mixed.reshape(seq_rows, heads * head_dim).astype(jnp.bfloat16), new_state)

def reference(tokens, state, route_ids, route_weights, norm_mix, w_query, w_forget, w_input, w_gate, lower_bound, head_gain, w_out, norm_ffn, expert_gate, expert_up, expert_down):
    resid = tokens.astype(jnp.float32)
    normed = rms_scale(resid, norm_mix).astype(jnp.bfloat16)
    projected = jnp.stack([jnp.dot(normed, weight, preferred_element_type=jnp.float32).astype(jnp.bfloat16) for weight in (w_query, w_forget, w_input, w_gate)])
    mixed, new_state = mixer_state(projected, state, lower_bound, head_gain)
    mixer_out = jnp.dot(mixed, w_out, preferred_element_type=jnp.float32).astype(jnp.bfloat16)
    middle = resid + mixer_out.astype(jnp.float32)
    normed_two = rms_scale(middle, norm_ffn).astype(jnp.bfloat16)
    matches = (route_ids[:, :, None] == jnp.arange(EXPERTS, dtype=jnp.int32)[None, None, :]).astype(jnp.float32)
    combined = lax.optimization_barrier(jnp.sum(route_weights.astype(jnp.float32)[:, :, None] * matches, axis=1))
    expert_total = jnp.zeros_like(middle)
    for expert in range(EXPERTS):
        gate_act = jnp.dot(normed_two, expert_gate[:, expert * FF:(expert + 1) * FF], preferred_element_type=jnp.float32)
        up_act = jnp.dot(normed_two, expert_up[:, expert * FF:(expert + 1) * FF], preferred_element_type=jnp.float32)
        hidden = (jax.nn.silu(gate_act) * up_act).astype(jnp.bfloat16)
        down_act = jnp.dot(hidden, expert_down[expert * FF:(expert + 1) * FF, :], preferred_element_type=jnp.float32)
        expert_total = expert_total + combined[:, expert:expert + 1] * down_act
    return ((middle + expert_total).astype(jnp.bfloat16), new_state)
```

```python
import functools

import jax
import jax.numpy as jnp
from jax import lax
from jax.experimental import pallas as pl
from jax.experimental.pallas import tpu as pltpu
from jax.sharding import PartitionSpec as P

FF = 7168
EXPERTS = 4
VMEM = 67043328

epsilon = 1e-06
F32 = jnp.float32
BF16 = jnp.bfloat16


def rms_scale(values, gain):
    return values * lax.rsqrt(jnp.mean(values * values, axis=-1, keepdims=True) + epsilon) * gain


def kernel(
    n,
    tokens,
    state,
    ids,
    weights,
    norm_mix_in,
    w_query,
    w_forget,
    w_input,
    w_gate,
    lower_bound_in,
    head_gain_in,
    w_out,
    norm_ffn_in,
    expert_gate,
    expert_up,
    expert_down,
    layer_out,
    st,
    tok_buf,
    norm_mix,
    lower_bound,
    head_gain,
    norm_ffn,
    wp,
    wo,
    wg,
    wu,
    wd,
    xn,
    pj_send,
    pj_buf,
    gates,
    mx_buf,
    col_buf,
    mid_buf,
    squares,
    acc_gate,
    acc_up,
    hid,
    ps,
    fw,
    summed,
    ret_buf,
    load_sem,
    send_sem,
    recv_sem,
):
    me = lax.axis_index("ep")
    rows, width = tokens.shape
    heads, dim = state.shape[1], state.shape[2]
    cols = w_query.shape[1]
    total = n * rows
    hidden = expert_gate.shape[1]
    group = n // EXPERTS // 2
    both = 2 * rows

    loads = [pltpu.make_async_copy(tokens, tok_buf.at[me], load_sem.at[0])]
    for j, w in enumerate((w_query, w_forget, w_input, w_gate)):
        loads.append(pltpu.make_async_copy(w, wp.at[j], load_sem.at[1 + j]))
    loads.append(pltpu.make_async_copy(state, st, load_sem.at[5]))
    loads.append(pltpu.make_async_copy(w_out, wo, load_sem.at[6]))
    loads.append(pltpu.make_async_copy(expert_gate, wg, load_sem.at[7]))
    loads.append(pltpu.make_async_copy(expert_up, wu, load_sem.at[8]))
    loads.append(pltpu.make_async_copy(expert_down, wd, load_sem.at[9]))
    small = [
        pltpu.make_async_copy(a, b, load_sem.at[10 + j])
        for j, (a, b) in enumerate(
            (
                (norm_mix_in, norm_mix),
                (lower_bound_in, lower_bound),
                (head_gain_in, head_gain),
                (norm_ffn_in, norm_ffn),
            )
        )
    ]

    core = lax.rem(me, 2)
    chip = me // 2
    chips = n // 2
    partner = me + 1 - 2 * core

    def flip(index, k):
        bit = 1
        while bit <= k:
            if k & bit:
                index = index + bit * (1 - 2 * lax.rem(index // bit, 2))
            bit *= 2
        return index

    at = [flip(chip, k) for k in range(chips)]
    same = [2 * at[k] + core for k in range(chips)]
    cross = [2 * at[k] + 1 - core for k in range(chips)]
    far_first = list(range(chips - 1, 0, -1))

    barrier = pltpu.get_barrier_semaphore()
    for k in far_first + [0]:
        for peer in (same[k], cross[k]) if k else (partner,):
            pl.semaphore_signal(
                barrier, inc=1, device_id={"ep": peer}, device_id_type=pl.DeviceIdType.MESH
            )
    for load in loads[:1] + small + loads[1:]:
        load.start()
    pl.semaphore_wait(barrier, n - 1)
    sent = []

    def send(phase, slot, source, target, peer):
        copy = pltpu.make_async_remote_copy(
            src_ref=source,
            dst_ref=target,
            send_sem=send_sem.at[phase, slot],
            recv_sem=recv_sem.at[phase, slot],
            device_id={"ep": peer},
            device_id_type=pl.DeviceIdType.MESH,
        )
        copy.start()
        sent.append(copy)
        return copy

    def spread(phase, buf):
        block = buf.at[me]
        direct = {k: send(phase, k, block, block, cross[k]) for k in far_first}
        return direct, {0: send(phase, 0, block, block, partner)}

    def forward(phase, buf, copies, ks):
        direct, passed = copies
        for k in ks:
            if k:
                direct[k].wait_recv()
                block = buf.at[cross[k]]
                passed[k] = send(phase, chips + k, block, block, partner)

    def arrive(copies, ks):
        for k in ks:
            copies[1][k].wait_recv()

    def batches(count):
        inner = [[i, i + 1] for i in range(1, count - 1, 2)]
        return [[0]] + inner + ([[count - 1]] if count > 1 else [])

    def chip_rows(buf, k):
        return [buf[2 * at[k] + c].astype(F32) for c in range(2)]

    loads[0].wait()
    copies = spread(0, tok_buf)
    for load in small:
        load.wait()
    pairs = [[2 * j, 2 * j + 1] for j in range(chips // 2)]

    def norm_pair(ks):
        x = jnp.concatenate([part for k in ks for part in chip_rows(tok_buf, k)], axis=0)
        for i, k in enumerate(ks):
            mid_buf[at[k]] = x[i * both : (i + 1) * both, :]
        xn[ks[0] * both : (ks[0] + 2) * both, :] = rms_scale(x, norm_mix[...]).astype(BF16)

    for j, ks in enumerate(pairs):
        forward(0, tok_buf, copies, ks)
        if j:
            arrive(copies, pairs[j - 1])
            norm_pair(pairs[j - 1])
    arrive(copies, pairs[-1])
    norm_pair(pairs[-1])

    for load in loads[1:5]:
        load.wait()
    w_all = jnp.concatenate([wp[j] for j in range(4)], axis=1)
    acc = jnp.dot(xn[...], w_all, preferred_element_type=F32)
    for s in range(n):
        pj_send[s] = acc[s * rows : (s + 1) * rows, :].astype(BF16)
    moved = {}
    for k in far_first + [0]:
        for r, peer in enumerate((same[k], cross[k])):
            if k or r:
                source = pj_send.at[2 * k + (core if r == 0 else 1 - core)]
                moved[k, r] = send(1, 2 * k + r, source, pj_buf.at[me], peer)
    pj_buf[me] = pj_send[core]

    per_head = max(1, dim // cols)
    head_chips = max(1, per_head // 2)
    chip_heads = head_chips * 2 * cols // dim
    loads[5].wait()

    def head_step(h, first):
        def owned(j):
            return jnp.concatenate(
                [
                    pj_buf[first + i][:, j * cols : (j + 1) * cols].astype(F32)
                    for i in range(per_head)
                ],
                axis=1,
            )

        bound = lower_bound[h]
        forget_raw = owned(1)
        decay = bound + (1.0 - bound) * jax.nn.sigmoid(forget_raw)
        key_vec = (1.0 - bound) * jax.nn.sigmoid(-forget_raw)
        query_vec = jax.nn.silu(owned(0)) * dim ** (-0.5)
        input_raw = owned(2)
        flat = jnp.concatenate([query_vec * decay, decay, key_vec, input_raw], axis=0)
        gates[h] = flat
        turned = flat.T
        out = [
            jnp.sum(turned[:, t : t + 1] * st[t, h], axis=0, keepdims=True) for t in range(rows)
        ]
        read = jnp.concatenate(out, axis=0) + input_raw * jnp.sum(
            query_vec * key_vec, axis=1, keepdims=True
        )
        mixed = rms_scale(read, head_gain[...]) * jax.nn.silu(owned(3))
        part = pl.ds(pl.multiple_of(h * dim, dim), dim)
        mx_buf[me, :, part] = mixed.astype(BF16)

    for batch in batches(chips // head_chips):
        for m in batch:
            for k in range(m * head_chips, (m + 1) * head_chips):
                for r in range(2):
                    if k or r:
                        moved[k, r].wait_recv()
        for m in batch:
            base = flip(chip // head_chips, m)
            for i in range(chip_heads):
                head_step(base * chip_heads + i, base * head_chips * 2 + i * per_head)

    def update_step(h, carry):
        flat = gates[h]
        turned = flat.T
        for t in range(rows):
            st[t, h] = (
                turned[:, rows + t : rows + t + 1] * st[t, h]
                + turned[:, 2 * rows + t : 2 * rows + t + 1]
                * flat[3 * rows + t : 3 * rows + t + 1, :]
            )
        return carry

    first_part = heads * 5 // 8
    second_part = heads * 7 // 8

    copies = spread(2, mx_buf)
    loads[6].wait()
    lax.fori_loop(0, first_part, update_step, 0, unroll=2)

    def gather_pair(ks):
        x = jnp.concatenate([part for k in ks for part in chip_rows(mx_buf, k)], axis=0)
        xn[ks[0] * both : (ks[0] + 2) * both, :] = x.astype(BF16)

    for j, ks in enumerate(pairs):
        forward(2, mx_buf, copies, ks)
        if j:
            arrive(copies, pairs[j - 1])
            gather_pair(pairs[j - 1])
    arrive(copies, pairs[-1])
    gather_pair(pairs[-1])

    acc = jnp.dot(xn[...], wo[...], preferred_element_type=F32)
    for k in range(chips):
        col_buf[me, at[k]] = acc[k * both : (k + 1) * both, :].astype(BF16)

    copies = spread(3, col_buf)
    lax.fori_loop(first_part, second_part, update_step, 0, unroll=2)
    loads[7].wait()
    loads[8].wait()
    tile = 256 if hidden % 256 == 0 else hidden
    slab_chips = max(1, 256 // (2 * cols))
    slab = slab_chips * 2 * cols
    slabs = chips // slab_chips
    plan = batches(slabs)

    def slab_of(m):
        base = flip(chip // slab_chips, m)
        first = base * slab_chips * 2
        part = pl.ds(pl.multiple_of(base * slab, slab), slab)
        y = jnp.concatenate(
            [col_buf[first + i].astype(F32) for i in range(2 * slab_chips)], axis=2
        )
        middle = mid_buf[:, :, part] + y
        mid_buf[:, :, part] = middle
        scaled = (middle * norm_ffn[:, part]).reshape(total, slab).astype(BF16)
        return part, scaled, jnp.sum((middle * middle).reshape(total, slab), axis=1, keepdims=True)

    def members(batch):
        return [k for m in batch for k in range(m * slab_chips, (m + 1) * slab_chips)]

    for b, batch in enumerate(plan):
        if b == 0:
            forward(3, col_buf, copies, members(batch))
        if b + 1 < len(plan) and b > 0:
            forward(3, col_buf, copies, members(plan[b + 1]))
        if b == 0 and len(plan) > 1:
            arrive(copies, members(batch))
        else:
            arrive(copies, members(batch))
        ready = [slab_of(m) for m in batch]
        power = sum(r[2] for r in ready)
        if b:
            power = power + squares[...]
        last = b + 1 == len(plan)
        if last:
            scale = lax.rsqrt(power / width + epsilon)
        else:
            squares[...] = power
        for j in range(hidden // tile):
            span = slice(j * tile, (j + 1) * tile)
            g = sum(jnp.dot(r[1], wg[r[0], span], preferred_element_type=F32) for r in ready)
            u = sum(jnp.dot(r[1], wu[r[0], span], preferred_element_type=F32) for r in ready)
            if b:
                g = g + acc_gate[:, span]
                u = u + acc_up[:, span]
            if last:
                hid[:, span] = (jax.nn.silu(g * scale) * (u * scale)).astype(BF16)
            else:
                acc_gate[:, span] = g
                acc_up[:, span] = u
        if b == 0 and len(plan) > 1:
            forward(3, col_buf, copies, members(plan[1]))

    loads[9].wait()
    out_tile = 256
    pieces = 4
    piece = width // pieces

    halves = []
    for p in range(pieces):
        for q in range(piece // out_tile):
            part = slice(p * piece + q * out_tile, p * piece + (q + 1) * out_tile)
            d = jnp.dot(hid[...], wd[:, part], preferred_element_type=F32)
            for s in range(n):
                ps[s % 2, s // 2, :, part] = d[s * rows : (s + 1) * rows, :].astype(BF16)
        part = pl.ds(p * piece, piece)
        halves.append(send(4, p, ps.at[core, :, :, part], fw.at[:, :, part], partner))
    returns = []
    for p in range(pieces):
        part = pl.ds(p * piece, piece)
        halves[p].wait_recv()
        for c in range(chips):
            summed[c, :, part] = (
                ps[1 - core, c, :, part].astype(F32) + fw[c, :, part].astype(F32)
            ).astype(BF16)
        for k in far_first + [0]:
            returns.append(
                send(
                    5 + p,
                    k,
                    summed.at[at[k], :, part],
                    ret_buf.at[chip, :, part],
                    cross[k],
                )
            )
    lax.fori_loop(second_part, heads, update_step, 0, unroll=2)
    for copy in returns:
        copy.wait_recv()
    own = mid_buf[chip]
    result = jnp.where(core == 0, own[:rows, :], own[rows:, :])
    diagonal = lax.broadcasted_iota(jnp.int32, (rows, rows), 0) == lax.broadcasted_iota(
        jnp.int32, (rows, rows), 1
    )
    for e in range(EXPERTS):
        flat_share = jnp.sum(
            jnp.where(ids[...] == e, weights[...].astype(F32), 0.0), axis=0, keepdims=True
        )
        share = jnp.sum(jnp.where(diagonal, flat_share, 0.0), axis=1, keepdims=True)
        rows_e = ret_buf[e * group].astype(F32)
        for s in range(1, group):
            rows_e = rows_e + ret_buf[e * group + s].astype(F32)
        result = result + share * rows_e
    layer_out[...] = result.astype(BF16)

    for copy in sent:
        copy.wait_send()


def local(n, *args):
    (
        tokens,
        state,
        ids,
        weights,
        norm_mix,
        w_query,
        w_forget,
        w_input,
        w_gate,
        lower_bound,
        head_gain,
        w_out,
        norm_ffn,
        expert_gate,
        expert_up,
        expert_down,
    ) = args
    rows, width = tokens.shape
    heads, dim = state.shape[1], state.shape[2]
    cols = w_query.shape[1]
    hidden = expert_gate.shape[1]
    total = n * rows
    any_spec = pl.BlockSpec(memory_space=pltpu.HBM)
    vmem = pl.BlockSpec(memory_space=pltpu.VMEM)
    return pl.pallas_call(
        functools.partial(kernel, n),
        out_shape=(
            pltpu.VMEM(tokens.shape, tokens.dtype),
            pltpu.VMEM(state.shape, state.dtype),
        ),
        in_specs=[any_spec, any_spec, vmem, vmem] + [any_spec] * 12,
        out_specs=(vmem, vmem),
        scratch_shapes=[
            pltpu.VMEM((n, rows, width), BF16),
            pltpu.VMEM((1, width), F32),
            pltpu.VMEM((heads, 1, dim), F32),
            pltpu.VMEM((1, dim), F32),
            pltpu.VMEM((1, width), F32),
            pltpu.VMEM((4, width, cols), BF16),
            pltpu.VMEM((width, cols), BF16),
            pltpu.VMEM((width, hidden), BF16),
            pltpu.VMEM((width, hidden), BF16),
            pltpu.VMEM((hidden, width), BF16),
            pltpu.VMEM((total, width), BF16),
            pltpu.VMEM((n, rows, 4 * cols), BF16),
            pltpu.VMEM((n, rows, 4 * cols), BF16),
            pltpu.VMEM((heads, 4 * rows, dim), F32),
            pltpu.VMEM((n, rows, width), BF16),
            pltpu.VMEM((n, n // 2, 2 * rows, cols), BF16),
            pltpu.VMEM((n // 2, 2 * rows, width), F32),
            pltpu.VMEM((total, 1), F32),
            pltpu.VMEM((total, hidden), F32),
            pltpu.VMEM((total, hidden), F32),
            pltpu.VMEM((total, hidden), BF16),
            pltpu.VMEM((2, n // 2, rows, width), BF16),
            pltpu.VMEM((n // 2, rows, width), BF16),
            pltpu.VMEM((n // 2, rows, width), BF16),
            pltpu.VMEM((n // 2, rows, width), BF16),
            pltpu.SemaphoreType.DMA((14,)),
            pltpu.SemaphoreType.DMA((9, n)),
            pltpu.SemaphoreType.DMA((9, n)),
        ],
        compiler_params=pltpu.CompilerParams(
            collective_id=0,
            has_side_effects=True,
            vmem_limit_bytes=VMEM - 4 * state.size - 64 * 1024,
        ),
    )(
        tokens,
        state,
        ids.T,
        weights.T,
        norm_mix[None],
        w_query,
        w_forget,
        w_input,
        w_gate,
        lower_bound.reshape(heads, 1, dim),
        head_gain[None],
        w_out,
        norm_ffn[None],
        expert_gate,
        expert_up,
        expert_down,
    )


def solution(mesh):
    return jax.shard_map(
        functools.partial(local, mesh.shape["ep"]),
        mesh=mesh,
        in_specs=(
            P(("grp", "ep"), None),
            P(("grp", "ep"), None, None, None),
            P(("grp", "ep"), None),
            P(("grp", "ep"), None),
            P(),
            P(None, "ep"),
            P(None, "ep"),
            P(None, "ep"),
            P(None, "ep"),
            P(),
            P(),
            P(None, "ep"),
            P(),
            P(None, "ep"),
            P(None, "ep"),
            P("ep", None),
        ),
        out_specs=(P(("grp", "ep"), None), P(("grp", "ep"), None, None, None)),
        check_vma=False,
    )
```

```python
import functools

import jax
import jax.numpy as jnp
from jax import lax
from jax.experimental import pallas as pl
from jax.experimental.pallas import tpu as pltpu
from jax.sharding import PartitionSpec as P

FF = 7168
EXPERTS = 4
VMEM = 67043328

epsilon = 1e-06
F32 = jnp.float32
BF16 = jnp.bfloat16


def rms_scale(values, gain):
    return values * lax.rsqrt(jnp.mean(values * values, axis=-1, keepdims=True) + epsilon) * gain


def kernel(
    n,
    tokens,
    state,
    ids,
    weights,
    norm_mix_in,
    w_query,
    w_forget,
    w_input,
    w_gate,
    lower_bound_in,
    head_gain_in,
    w_out,
    norm_ffn_in,
    expert_gate,
    expert_up,
    expert_down,
    layer_out,
    st,
    tok_buf,
    norm_mix,
    lower_bound,
    head_gain,
    norm_ffn,
    wp,
    wo,
    wg,
    wu,
    wd,
    xn,
    pj_send,
    pj_buf,
    gates,
    mx_buf,
    col_buf,
    mid_buf,
    squares,
    acc_gate,
    acc_up,
    hid,
    ps,
    fw,
    summed,
    ret_buf,
    load_sem,
    send_sem,
    recv_sem,
    late_sem,
):
    me = lax.axis_index("ep")
    rows, width = tokens.shape
    heads, dim = state.shape[1], state.shape[2]
    cols = w_query.shape[1]
    total = n * rows
    hidden = expert_gate.shape[1]
    group = n // EXPERTS // 2
    both = 2 * rows

    loads = [pltpu.make_async_copy(tokens, tok_buf.at[me], load_sem.at[0])]
    for j, w in enumerate((w_query, w_forget, w_input, w_gate)):
        loads.append(pltpu.make_async_copy(w, wp.at[j], load_sem.at[1 + j]))
    loads.append(pltpu.make_async_copy(state, st, load_sem.at[5]))
    loads.append(pltpu.make_async_copy(w_out, wo, load_sem.at[6]))
    loads.append(pltpu.make_async_copy(expert_gate, wg, load_sem.at[7]))
    loads.append(pltpu.make_async_copy(expert_up, wu, load_sem.at[8]))
    loads.append(pltpu.make_async_copy(expert_down, wd, load_sem.at[9]))
    small = [
        pltpu.make_async_copy(a, b, load_sem.at[10 + j])
        for j, (a, b) in enumerate(
            (
                (norm_mix_in, norm_mix),
                (lower_bound_in, lower_bound),
                (head_gain_in, head_gain),
                (norm_ffn_in, norm_ffn),
            )
        )
    ]

    core = lax.rem(me, 2)
    chip = me // 2
    chips = n // 2
    partner = me + 1 - 2 * core

    def flip(index, k):
        bit = 1
        while bit <= k:
            if k & bit:
                index = index + bit * (1 - 2 * lax.rem(index // bit, 2))
            bit *= 2
        return index

    bits = [1 << b for b in range(chips.bit_length() - 1)]
    at = [flip(chip, k) for k in range(chips)]
    same = [2 * at[k] + core for k in range(chips)]
    cross = [2 * at[k] + 1 - core for k in range(chips)]
    far_first = list(range(chips - 1, 0, -1))
    barrier = pltpu.get_barrier_semaphore()
    late = chip == chips - 1

    def signal(semaphore, peer):
        pl.semaphore_signal(
            semaphore, inc=1, device_id={"ep": peer}, device_id_type=pl.DeviceIdType.MESH
        )

    @pl.when(late)
    def _():
        signal(barrier, partner)

    @pl.when(jnp.logical_not(late))
    def _():
        for k in far_first:
            signal(barrier, same[k])
            signal(barrier, cross[k])
        signal(barrier, partner)

    loads[0].start()

    @pl.when(late)
    def _():
        pl.semaphore_wait(barrier, n - 1)
        for k in far_first:
            signal(late_sem, same[k])
            signal(late_sem, cross[k])

    for load in small + loads[1:]:
        load.start()

    @pl.when(jnp.logical_not(late))
    def _():
        pl.semaphore_wait(barrier, n - 3)

    sent = []

    def handle(phase, slot, source, target, peer):
        return pltpu.make_async_remote_copy(
            src_ref=source,
            dst_ref=target,
            send_sem=send_sem.at[phase, slot],
            recv_sem=recv_sem.at[phase, slot],
            device_id={"ep": peer},
            device_id_type=pl.DeviceIdType.MESH,
        )

    def send(phase, slot, source, target, peer):
        copy = handle(phase, slot, source, target, peer)
        copy.start()
        sent.append(copy)
        return copy

    def scatter(phase, block, near=0, order=None):
        return {
            k: (
                [send(phase, k, block, block, cross[k])]
                + ([send(phase, chips + k, block, block, same[k])] if k <= near else [])
            )
            for k in order or far_first
        }

    def forward(phase, buf, copies, passed, ks, near=0):
        for k in ks:
            for part in copies:
                if k:
                    for copy in part[k]:
                        copy.wait_recv()
            if k == 0:
                passed[k] = send(phase, 0, buf.at[me], buf.at[me], partner)
            elif k > near:
                block = buf.at[cross[k]]
                passed[k] = send(phase, chips + k, block, block, partner)

    def arrive(passed, ks):
        for k in ks:
            if k in passed:
                passed[k].wait_recv()

    shares = [(0, chips // 2), (chips // 2, chips * 3 // 4), (chips * 3 // 4, chips)]

    def base_of(index, lo, hi):
        return flip(index // (hi - lo), lo // (hi - lo)) * (hi - lo)

    def chip_rows(buf, k):
        return [buf[2 * at[k] + c].astype(F32) for c in range(2)]
    loads[0].wait()
    own = tok_buf.at[me]
    to_late = sum(bit * (1 - lax.rem(chip // bit, 2)) for bit in bits)
    direct = [handle(0, k, own, own, cross[k] if k else partner) for k in range(chips)]
    extra = pltpu.make_async_remote_copy(
        src_ref=own,
        dst_ref=own,
        send_sem=send_sem.at[7, 0],
        recv_sem=recv_sem.at[0, chips + to_late],
        device_id={"ep": n - 2 + core},
        device_id_type=pl.DeviceIdType.MESH,
    )
    for k in far_first:

        @pl.when(at[k] != chips - 1)
        def _(k=k):
            direct[k].start()

    @pl.when(jnp.logical_not(late))
    def _():
        direct[0].start()
        pl.semaphore_wait(late_sem, 2)
        extra.start()

    handle(0, to_late, own, own, n - 1 - core).start()
    sent.extend(direct)
    through = []

    for load in small:
        load.wait()
    pairs = [[2 * j, 2 * j + 1] for j in range(chips // 2)]

    def norm_pair(ks):
        x = jnp.concatenate([part for k in ks for part in chip_rows(tok_buf, k)], axis=0)
        for i, k in enumerate(ks):
            mid_buf[at[k]] = x[i * both : (i + 1) * both, :]
        xn[ks[0] * both : (ks[0] + 2) * both, :] = rms_scale(x, norm_mix[...]).astype(BF16)

    def pass_on(k):
        direct[k].wait_recv()
        block = tok_buf.at[cross[k]]
        through.append(handle(0, chips + k, block, block, partner))

        @pl.when(jnp.logical_not(late))
        def _():
            through[-1].start()

    def settle_pair(ks):
        for k in ks:
            (through[k - 1] if k else direct[0]).wait_recv()
        norm_pair(ks)

    for j, ks in enumerate(pairs):
        for k in ks:
            if k:
                pass_on(k)
        if j:
            settle_pair(pairs[j - 1])
    settle_pair(pairs[-1])
    for load in loads[1:5]:
        load.wait()
    w_all = jnp.concatenate([wp[j] for j in range(4)], axis=1)
    acc = jnp.dot(xn[...], w_all, preferred_element_type=F32)
    for s in range(n):
        pj_send[s] = acc[s * rows : (s + 1) * rows, :].astype(BF16)
    moved = {}
    for k in far_first + [0]:
        for r, peer in enumerate((same[k], cross[k])):
            if k or r:
                source = pj_send.at[2 * k + (core if r == 0 else 1 - core)]
                moved[k, r] = send(1, 2 * k + r, source, pj_buf.at[me], peer)
    pj_buf[me] = pj_send[core]
    per_head = max(1, dim // cols)
    head_chips = max(1, per_head // 2)
    chip_heads = head_chips * 2 * cols // dim
    loads[5].wait()

    def head_step(h, first):
        def owned(j):
            return jnp.concatenate(
                [
                    pj_buf[first + i][:, j * cols : (j + 1) * cols].astype(F32)
                    for i in range(per_head)
                ],
                axis=1,
            )

        bound = lower_bound[h]
        forget_raw = owned(1)
        decay = bound + (1.0 - bound) * jax.nn.sigmoid(forget_raw)
        key_vec = (1.0 - bound) * jax.nn.sigmoid(-forget_raw)
        query_vec = jax.nn.silu(owned(0)) * dim ** (-0.5)
        input_raw = owned(2)
        read_vec = query_vec * decay
        gates[h] = jnp.concatenate([read_vec, decay, key_vec, input_raw], axis=0)
        wide = jnp.dot(
            read_vec,
            jnp.concatenate([st[t, h] for t in range(rows)], axis=1),
            preferred_element_type=F32,
        )
        read = jnp.concatenate(
            [wide[t : t + 1, t * dim : (t + 1) * dim] for t in range(rows)], axis=0
        ) + input_raw * jnp.sum(query_vec * key_vec, axis=1, keepdims=True)
        mixed = rms_scale(read, head_gain[...]) * jax.nn.silu(owned(3))
        part = pl.ds(pl.multiple_of(h * dim, dim), dim)
        mx_buf[me, :, part] = mixed.astype(BF16)

    mixed_parts = []
    for lo, hi in shares:
        step = max(2, head_chips)
        for first in range(lo, hi, step):
            for k in range(first, first + step):
                for r in range(2):
                    if k or r:
                        moved[k, r].wait_recv()
            for m in range(first // head_chips, (first + step) // head_chips):
                base = flip(chip // head_chips, m)
                for i in range(chip_heads):
                    head_step(base * chip_heads + i, base * head_chips * 2 + i * per_head)
        size = (hi - lo) * 2 * cols
        offset = pl.multiple_of(base_of(chip, lo, hi) * 2 * cols, size)
        mixed_parts.append(
            scatter(2 + len(mixed_parts), mx_buf.at[me, :, pl.ds(offset, size)])
        )

    def update_step(h, carry):
        flat = gates[h]
        turned = flat.T
        for t in range(rows):
            st[t, h] = (
                turned[:, rows + t : rows + t + 1] * st[t, h]
                + turned[:, 2 * rows + t : 2 * rows + t + 1]
                * flat[3 * rows + t : 3 * rows + t + 1, :]
            )
        return carry

    cuts = [heads * c // 16 for c in (0, 8, 11, 13, 16)]

    def update(c):
        lax.fori_loop(cuts[c], cuts[c + 1], update_step, 0, unroll=2)
    passed = {}
    forward(4, mx_buf, mixed_parts, passed, [0])
    loads[6].wait()
    update(0)
    near = min(1, chips - 1)
    col_parts = []

    def gather_pair(ks):
        arrive(passed, ks)
        x = jnp.concatenate([part for k in ks for part in chip_rows(mx_buf, k)], axis=0)
        xn[ks[0] * both : (ks[0] + 2) * both, :] = x.astype(BF16)

    def project(lo, hi):
        acc = jnp.dot(xn[lo * both : hi * both, :], wo[...], preferred_element_type=F32)
        for k in range(lo, hi):
            col_buf[me, at[k]] = acc[(k - lo) * both : (k - lo + 1) * both, :].astype(BF16)
        base = base_of(chip, lo, hi)
        col_parts.append(
            scatter(5 + len(col_parts), col_buf.at[me, pl.ds(base, hi - lo)], near, far_first[::-1])
        )

    for j, ks in enumerate(pairs):
        forward(4, mx_buf, mixed_parts, passed, [k for k in ks if k])
        if j:
            gather_pair(pairs[j - 1])
            ready = 2 * j
            if ready == chips // 2:
                project(0, ready)
    gather_pair(pairs[-1])
    project(chips // 2, chips)
    passed = {}
    forward(6, col_buf, col_parts, passed, [0])
    update(1)
    loads[7].wait()
    loads[8].wait()
    tile = 256 if hidden % 256 == 0 else hidden
    slab_chips = max(1, 256 // (2 * cols))
    slab = slab_chips * 2 * cols
    slabs = chips // slab_chips

    def slab_of(m):
        base = flip(chip // slab_chips, m)
        first = base * slab_chips * 2
        part = pl.ds(pl.multiple_of(base * slab, slab), slab)
        y = jnp.concatenate(
            [col_buf[first + i].astype(F32) for i in range(2 * slab_chips)], axis=2
        )
        middle = mid_buf[:, :, part] + y
        mid_buf[:, :, part] = middle
        scaled = (middle * norm_ffn[:, part]).reshape(total, slab).astype(BF16)
        return part, scaled, jnp.sum((middle * middle).reshape(total, slab), axis=1, keepdims=True)

    following = 1
    for m in range(slabs):
        ks = range(m * slab_chips, (m + 1) * slab_chips)
        ahead = m if m < 2 else min(2 * m, slabs - 1)
        forward(6, col_buf, col_parts, passed, range(following, (ahead + 1) * slab_chips), near)
        following = max(following, (ahead + 1) * slab_chips)
        arrive(passed, ks)
        part, scaled, power = slab_of(m)
        if m:
            power = power + squares[...]
        last = m + 1 == slabs
        if last:
            scale = lax.rsqrt(power / width + epsilon)
        else:
            squares[...] = power
        for j in range(hidden // tile):
            span = slice(j * tile, (j + 1) * tile)
            g = jnp.dot(scaled, wg[part, span], preferred_element_type=F32)
            u = jnp.dot(scaled, wu[part, span], preferred_element_type=F32)
            if m:
                g = g + acc_gate[:, span]
                u = u + acc_up[:, span]
            if last:
                hid[:, span] = (jax.nn.silu(g * scale) * (u * scale)).astype(BF16)
            else:
                acc_gate[:, span] = g
                acc_up[:, span] = u
        if m == 0:
            update(2)
    loads[9].wait()
    out_tile = 256
    pieces = 4
    piece = width // pieces

    halves, returns = [], []

    def settle(p):
        part = pl.ds(p * piece, piece)
        halves[p].wait_recv()
        for c in range(chips):
            summed[c, :, part] = (
                ps[1 - core, c, :, part].astype(F32) + fw[c, :, part].astype(F32)
            ).astype(BF16)
        for k in far_first + [0]:
            returns.append(
                send(
                    9 + p,
                    k,
                    summed.at[at[k], :, part],
                    ret_buf.at[chip, :, part],
                    cross[k],
                )
            )

    for p in range(pieces):
        for q in range(piece // out_tile):
            part = slice(p * piece + q * out_tile, p * piece + (q + 1) * out_tile)
            d = jnp.dot(hid[...], wd[:, part], preferred_element_type=F32)
            for s in range(n):
                ps[s % 2, s // 2, :, part] = d[s * rows : (s + 1) * rows, :].astype(BF16)
        part = pl.ds(p * piece, piece)
        halves.append(send(8, p, ps.at[core, :, :, part], fw.at[:, :, part], partner))
        if p >= 2:
            settle(p - 2)
    for p in range(pieces - 2, pieces):
        settle(p)
    update(3)
    for copy in returns:
        copy.wait_recv()
    own = mid_buf[chip]
    result = jnp.where(core == 0, own[:rows, :], own[rows:, :])
    diagonal = lax.broadcasted_iota(jnp.int32, (rows, rows), 0) == lax.broadcasted_iota(
        jnp.int32, (rows, rows), 1
    )
    for e in range(EXPERTS):
        flat_share = jnp.sum(
            jnp.where(ids[...] == e, weights[...].astype(F32), 0.0), axis=0, keepdims=True
        )
        share = jnp.sum(jnp.where(diagonal, flat_share, 0.0), axis=1, keepdims=True)
        rows_e = ret_buf[e * group].astype(F32)
        for s in range(1, group):
            rows_e = rows_e + ret_buf[e * group + s].astype(F32)
        result = result + share * rows_e
    layer_out[...] = result.astype(BF16)
    for copy in sent:
        copy.wait_send()

    @pl.when(jnp.logical_not(late))
    def _():
        extra.wait_send()
        for copy in through:
            copy.wait_send()


def write(layer_in, state_in, layer_out, state_out, sem):
    copies = [pltpu.make_async_copy(layer_in, layer_out, sem.at[0])]
    for t in range(state_in.shape[0]):
        copies.append(pltpu.make_async_copy(state_in.at[t], state_out.at[t], sem.at[1 + t]))
    for copy in copies:
        copy.start()
    for copy in copies:
        copy.wait()


def local(n, *args):
    (
        tokens,
        state,
        ids,
        weights,
        norm_mix,
        w_query,
        w_forget,
        w_input,
        w_gate,
        lower_bound,
        head_gain,
        w_out,
        norm_ffn,
        expert_gate,
        expert_up,
        expert_down,
    ) = args
    rows, width = tokens.shape
    heads, dim = state.shape[1], state.shape[2]
    cols = w_query.shape[1]
    hidden = expert_gate.shape[1]
    total = n * rows
    any_spec = pl.BlockSpec(memory_space=pltpu.HBM)
    vmem = pl.BlockSpec(memory_space=pltpu.VMEM)
    layer, fresh = pl.pallas_call(
        functools.partial(kernel, n),
        out_shape=(
            pltpu.VMEM(tokens.shape, tokens.dtype),
            pltpu.VMEM(state.shape, state.dtype),
        ),
        in_specs=[any_spec, any_spec, vmem, vmem] + [any_spec] * 12,
        out_specs=(vmem, vmem),
        scratch_shapes=[
            pltpu.VMEM((n, rows, width), BF16),
            pltpu.VMEM((1, width), F32),
            pltpu.VMEM((heads, 1, dim), F32),
            pltpu.VMEM((1, dim), F32),
            pltpu.VMEM((1, width), F32),
            pltpu.VMEM((4, width, cols), BF16),
            pltpu.VMEM((width, cols), BF16),
            pltpu.VMEM((width, hidden), BF16),
            pltpu.VMEM((width, hidden), BF16),
            pltpu.VMEM((hidden, width), BF16),
            pltpu.VMEM((total, width), BF16),
            pltpu.VMEM((n, rows, 4 * cols), BF16),
            pltpu.VMEM((n, rows, 4 * cols), BF16),
            pltpu.VMEM((heads, 4 * rows, dim), F32),
            pltpu.VMEM((n, rows, width), BF16),
            pltpu.VMEM((n, n // 2, 2 * rows, cols), BF16),
            pltpu.VMEM((n // 2, 2 * rows, width), F32),
            pltpu.VMEM((total, 1), F32),
            pltpu.VMEM((total, hidden), F32),
            pltpu.VMEM((total, hidden), F32),
            pltpu.VMEM((total, hidden), BF16),
            pltpu.VMEM((2, n // 2, rows, width), BF16),
            pltpu.VMEM((n // 2, rows, width), BF16),
            pltpu.VMEM((n // 2, rows, width), BF16),
            pltpu.VMEM((n // 2, rows, width), BF16),
            pltpu.SemaphoreType.DMA((14,)),
            pltpu.SemaphoreType.DMA((13, n)),
            pltpu.SemaphoreType.DMA((13, n)),
            pltpu.SemaphoreType.REGULAR,
        ],
        compiler_params=pltpu.CompilerParams(
            collective_id=0,
            has_side_effects=True,
            vmem_limit_bytes=VMEM - 4 * state.size - 64 * 1024,
        ),
    )(
        tokens,
        state,
        ids.T,
        weights.T,
        norm_mix[None],
        w_query,
        w_forget,
        w_input,
        w_gate,
        lower_bound.reshape(heads, 1, dim),
        head_gain[None],
        w_out,
        norm_ffn[None],
        expert_gate,
        expert_up,
        expert_down,
    )
    return pl.pallas_call(
        write,
        out_shape=(
            jax.ShapeDtypeStruct(layer.shape, layer.dtype),
            jax.ShapeDtypeStruct(fresh.shape, fresh.dtype),
        ),
        in_specs=[vmem, vmem],
        out_specs=(any_spec, any_spec),
        scratch_shapes=[pltpu.SemaphoreType.DMA((1 + rows,))],
        compiler_params=pltpu.CompilerParams(vmem_limit_bytes=1 << 20),
    )(
        pltpu.with_memory_space_constraint(layer, pltpu.VMEM),
        pltpu.with_memory_space_constraint(fresh, pltpu.VMEM),
    )


def solution(mesh):
    return jax.shard_map(
        functools.partial(local, mesh.shape["ep"]),
        mesh=mesh,
        in_specs=(
            P(("grp", "ep"), None),
            P(("grp", "ep"), None, None, None),
            P(("grp", "ep"), None),
            P(("grp", "ep"), None),
            P(),
            P(None, "ep"),
            P(None, "ep"),
            P(None, "ep"),
            P(None, "ep"),
            P(),
            P(),
            P(None, "ep"),
            P(),
            P(None, "ep"),
            P(None, "ep"),
            P("ep", None),
        ),
        out_specs=(P(("grp", "ep"), None), P(("grp", "ep"), None, None, None)),
        check_vma=False,
    )
```

```python
import functools

import jax
import jax.numpy as jnp
from jax import lax
from jax.experimental import pallas as pl
from jax.experimental.pallas import tpu as pltpu
from jax.sharding import PartitionSpec as P

FF = 7168
EXPERTS = 4
VMEM = 67043328

epsilon = 1e-06
F32 = jnp.float32
BF16 = jnp.bfloat16


def rms_scale(values, gain):
    return values * lax.rsqrt(jnp.mean(values * values, axis=-1, keepdims=True) + epsilon) * gain


def kernel(
    n,
    tokens,
    state,
    ids_in,
    weights_in,
    norm_mix_in,
    w_query,
    w_forget,
    w_input,
    w_gate,
    lower_bound_in,
    head_gain_in,
    w_out,
    norm_ffn_in,
    expert_gate,
    expert_up,
    expert_down,
    layer_out,
    st,
    tok_buf,
    norm_mix,
    lower_bound,
    head_gain,
    norm_ffn,
    wp,
    wo,
    wg,
    wu,
    wd,
    xn,
    pj_send,
    pj_buf,
    gates,
    mx_buf,
    col_buf,
    mid_buf,
    squares,
    acc_gate,
    acc_up,
    hid,
    ps,
    fw,
    summed,
    ret_buf,
    ids,
    weights,
    load_sem,
    send_sem,
    recv_sem,
    late_sem,
):
    me = lax.axis_index("ep")
    rows, width = tokens.shape
    heads, dim = state.shape[1], state.shape[2]
    cols = w_query.shape[1]
    total = n * rows
    hidden = expert_gate.shape[1]
    group = n // EXPERTS // 2
    both = 2 * rows

    loads = [pltpu.make_async_copy(tokens, tok_buf.at[me], load_sem.at[0])]
    for j, w in enumerate((w_query, w_forget, w_input, w_gate)):
        loads.append(pltpu.make_async_copy(w, wp.at[j], load_sem.at[1 + j]))
    loads.append(pltpu.make_async_copy(state, st, load_sem.at[5]))
    loads.append(pltpu.make_async_copy(w_out, wo, load_sem.at[6]))
    loads.append(pltpu.make_async_copy(expert_gate, wg, load_sem.at[7]))
    loads.append(pltpu.make_async_copy(expert_up, wu, load_sem.at[8]))
    loads.append(pltpu.make_async_copy(expert_down, wd, load_sem.at[9]))
    loads.append(pltpu.make_async_copy(ids_in, ids, load_sem.at[14]))
    loads.append(pltpu.make_async_copy(weights_in, weights, load_sem.at[15]))
    small = [
        pltpu.make_async_copy(a, b, load_sem.at[10 + j])
        for j, (a, b) in enumerate(
            (
                (norm_mix_in, norm_mix),
                (lower_bound_in, lower_bound),
                (head_gain_in, head_gain),
                (norm_ffn_in, norm_ffn),
            )
        )
    ]

    core = lax.rem(me, 2)
    chip = me // 2
    chips = n // 2
    partner = me + 1 - 2 * core

    def flip(index, k):
        bit = 1
        while bit <= k:
            if k & bit:
                index = index + bit * (1 - 2 * lax.rem(index // bit, 2))
            bit *= 2
        return index

    bits = [1 << b for b in range(chips.bit_length() - 1)]
    at = [flip(chip, k) for k in range(chips)]
    same = [2 * at[k] + core for k in range(chips)]
    cross = [2 * at[k] + 1 - core for k in range(chips)]
    far_first = list(range(chips - 1, 0, -1))
    barrier = pltpu.get_barrier_semaphore()
    late = chip == chips - 1

    def signal(semaphore, peer):
        pl.semaphore_signal(
            semaphore, inc=1, device_id={"ep": peer}, device_id_type=pl.DeviceIdType.MESH
        )

    @pl.when(late)
    def _():
        signal(barrier, partner)

    @pl.when(jnp.logical_not(late))
    def _():
        for k in far_first:
            signal(barrier, same[k])
            signal(barrier, cross[k])
        signal(barrier, partner)

    loads[0].start()

    @pl.when(late)
    def _():
        pl.semaphore_wait(barrier, n - 1)
        for k in far_first:
            signal(late_sem, same[k])
            signal(late_sem, cross[k])

    for load in small + loads[1:]:
        load.start()

    @pl.when(jnp.logical_not(late))
    def _():
        pl.semaphore_wait(barrier, n - 3)

    GATHER, MOVE, MIXED, COLUMNS, PAIR, RETURN = range(6)

    def lane(phase, slot, direct):
        if phase == MOVE or (phase == COLUMNS and not direct):
            return n + slot
        if phase == PAIR or (phase == MIXED and direct):
            return 2 * n + slot
        return 2 * n + chips if phase == RETURN else slot

    def handle(phase, slot, source, target, peer, direct=False):
        return pltpu.make_async_remote_copy(
            src_ref=source,
            dst_ref=target,
            send_sem=send_sem.at[phase],
            recv_sem=recv_sem.at[lane(phase, slot, direct)],
            device_id={"ep": peer},
            device_id_type=pl.DeviceIdType.MESH,
        )

    def send(phase, slot, source, target, peer, direct=False):
        copy = handle(phase, slot, source, target, peer, direct)
        copy.start()
        return copy

    def whole(phase, slot, block, direct=False):
        return handle(phase, slot, block, block, partner, direct)

    def scatter(phase, block, near=0):
        for k in far_first:
            send(phase, k, block, block, cross[k], True)
            if k <= near:
                send(phase, chips + k, block, block, same[k])

    def forward(phase, buf, passed, ks, near=0):
        for k in ks:
            if k == 0:
                passed[k] = send(phase, 0, buf.at[me], buf.at[me], partner)
            else:
                block = buf.at[cross[k]]
                whole(phase, k, block, True).wait_recv()
                if k > near:
                    passed[k] = send(phase, chips + k, block, block, partner)
                else:
                    whole(phase, chips + k, buf.at[same[k]]).wait_recv()

    def arrive(passed, ks):
        for k in ks:
            if k in passed:
                passed[k].wait_recv()

    shares = [(0, chips // 2), (chips // 2, chips * 3 // 4), (chips * 3 // 4, chips)]

    def base_of(index, lo, hi):
        return flip(index // (hi - lo), lo // (hi - lo)) * (hi - lo)

    def chip_rows(buf, k):
        return [buf[2 * at[k] + c].astype(F32) for c in range(2)]
    loads[0].wait()
    own = tok_buf.at[me]
    to_late = sum(bit * (1 - lax.rem(chip // bit, 2)) for bit in bits)
    direct = [handle(0, k, own, own, cross[k] if k else partner) for k in range(chips)]
    extra = pltpu.make_async_remote_copy(
        src_ref=own,
        dst_ref=own,
        send_sem=send_sem.at[GATHER],
        recv_sem=recv_sem.at[chips + to_late],
        device_id={"ep": n - 2 + core},
        device_id_type=pl.DeviceIdType.MESH,
    )
    for k in far_first:

        @pl.when(at[k] != chips - 1)
        def _(k=k):
            direct[k].start()

    @pl.when(jnp.logical_not(late))
    def _():
        direct[0].start()
        pl.semaphore_wait(late_sem, 2)
        extra.start()

    handle(0, to_late, own, own, n - 1 - core).start()
    through = []

    for load in small:
        load.wait()
    pairs = [[2 * j, 2 * j + 1] for j in range(chips // 2)]

    def norm_pair(ks):
        x = jnp.concatenate([part for k in ks for part in chip_rows(tok_buf, k)], axis=0)
        for i, k in enumerate(ks):
            mid_buf[at[k]] = x[i * both : (i + 1) * both, :]
        xn[ks[0] * both : (ks[0] + 2) * both, :] = rms_scale(x, norm_mix[...]).astype(BF16)

    def pass_on(k):
        direct[k].wait_recv()
        block = tok_buf.at[cross[k]]
        through.append(handle(0, chips + k, block, block, partner))

        @pl.when(jnp.logical_not(late))
        def _():
            through[-1].start()

    def settle_pair(ks):
        for k in ks:
            (through[k - 1] if k else direct[0]).wait_recv()
        norm_pair(ks)

    for j, ks in enumerate(pairs):
        for k in ks:
            if k:
                pass_on(k)
        if j:
            settle_pair(pairs[j - 1])
    settle_pair(pairs[-1])
    for load in loads[1:5]:
        load.wait()
    w_all = jnp.concatenate([wp[j] for j in range(4)], axis=1)
    acc = jnp.dot(xn[...], w_all, preferred_element_type=F32)
    for s in range(n):
        pj_send[s] = acc[s * rows : (s + 1) * rows, :].astype(BF16)
    moved = {}
    for k in far_first + [0]:
        for r, peer in enumerate((same[k], cross[k])):
            if k or r:
                source = pj_send.at[2 * k + (core if r == 0 else 1 - core)]
                moved[k, r] = send(MOVE, 2 * k + r, source, pj_buf.at[me], peer)
    pj_buf[me] = pj_send[core]
    per_head = max(1, dim // cols)
    head_chips = max(1, per_head // 2)
    chip_heads = head_chips * 2 * cols // dim
    loads[5].wait()

    def head_step(h, first):
        def owned(j):
            return jnp.concatenate(
                [
                    pj_buf[first + i][:, j * cols : (j + 1) * cols].astype(F32)
                    for i in range(per_head)
                ],
                axis=1,
            )

        bound = lower_bound[h]
        forget_raw = owned(1)
        decay = bound + (1.0 - bound) * jax.nn.sigmoid(forget_raw)
        key_vec = (1.0 - bound) * jax.nn.sigmoid(-forget_raw)
        query_vec = jax.nn.silu(owned(0)) * dim ** (-0.5)
        input_raw = owned(2)
        read_vec = query_vec * decay
        gates[h] = jnp.concatenate([read_vec, decay, key_vec, input_raw], axis=0)
        wide = jnp.dot(
            read_vec,
            jnp.concatenate([st[t, h] for t in range(rows)], axis=1),
            preferred_element_type=F32,
        )
        read = jnp.concatenate(
            [wide[t : t + 1, t * dim : (t + 1) * dim] for t in range(rows)], axis=0
        ) + input_raw * jnp.sum(query_vec * key_vec, axis=1, keepdims=True)
        mixed = rms_scale(read, head_gain[...]) * jax.nn.silu(owned(3))
        part = pl.ds(pl.multiple_of(h * dim, dim), dim)
        mx_buf[me, :, part] = mixed.astype(BF16)

    for lo, hi in shares:
        step = max(2, head_chips)
        for first in range(lo, hi, step):
            for k in range(first, first + step):
                for r in range(2):
                    if k or r:
                        moved[k, r].wait_recv()
            for m in range(first // head_chips, (first + step) // head_chips):
                base = flip(chip // head_chips, m)
                for i in range(chip_heads):
                    head_step(base * chip_heads + i, base * head_chips * 2 + i * per_head)
        size = (hi - lo) * 2 * cols
        offset = pl.multiple_of(base_of(chip, lo, hi) * 2 * cols, size)
        scatter(MIXED, mx_buf.at[me, :, pl.ds(offset, size)])

    def update_step(h, carry):
        flat = gates[h]
        turned = flat.T
        for t in range(rows):
            st[t, h] = (
                turned[:, rows + t : rows + t + 1] * st[t, h]
                + turned[:, 2 * rows + t : 2 * rows + t + 1]
                * flat[3 * rows + t : 3 * rows + t + 1, :]
            )
        return carry

    cuts = [heads * c // 16 for c in (0, 8, 11, 13, 16)]

    def update(c):
        lax.fori_loop(cuts[c], cuts[c + 1], update_step, 0, unroll=2)
    passed = {}
    forward(MIXED, mx_buf, passed, [0])
    loads[6].wait()
    update(0)
    near = min(1, chips - 1)

    def gather_pair(ks):
        arrive(passed, ks)
        x = jnp.concatenate([part for k in ks for part in chip_rows(mx_buf, k)], axis=0)
        xn[ks[0] * both : (ks[0] + 2) * both, :] = x.astype(BF16)

    def project(lo, hi):
        acc = jnp.dot(xn[lo * both : hi * both, :], wo[...], preferred_element_type=F32)
        for k in range(lo, hi):
            col_buf[me, at[k]] = acc[(k - lo) * both : (k - lo + 1) * both, :].astype(BF16)
        base = base_of(chip, lo, hi)
        scatter(COLUMNS, col_buf.at[me, pl.ds(base, hi - lo)], near)

    for j, ks in enumerate(pairs):
        forward(MIXED, mx_buf, passed, [k for k in ks if k])
        if j:
            gather_pair(pairs[j - 1])
            ready = 2 * j
            if ready == chips // 2:
                project(0, ready)
    gather_pair(pairs[-1])
    project(chips // 2, chips)
    passed = {}
    forward(COLUMNS, col_buf, passed, [0])
    update(1)
    loads[7].wait()
    loads[8].wait()
    tile = 256 if hidden % 256 == 0 else hidden
    slab_chips = max(1, 256 // (2 * cols))
    slab = slab_chips * 2 * cols
    slabs = chips // slab_chips

    def piece_of(first, count, offset, size):
        part = pl.ds(pl.multiple_of(offset, size), size)
        y = jnp.concatenate([col_buf[first + i].astype(F32) for i in range(count)], axis=2)
        middle = mid_buf[:, :, part] + y
        mid_buf[:, :, part] = middle
        scaled = (middle * norm_ffn[:, part]).reshape(total, size).astype(BF16)
        return part, scaled, jnp.sum((middle * middle).reshape(total, size), axis=1, keepdims=True)

    steps = []
    if cols % 128 == 0:

        def devices(peers):
            return [(peer, 1, peer * cols, cols) for peer in peers]

        steps.append(([], [0], [(2 * chip, 2, chip * slab, slab)]))
        if near:
            steps.append(([1], [], [(2 * at[1], 2, at[1] * slab, slab)]))
        rest = [[k, k + 1] for k in range(2 * near, chips, 2)]
        for ks in rest:
            steps.append((ks, [], devices(cross[k] for k in ks)))
        for ks in rest:
            steps.append(([], ks, devices(same[k] for k in ks)))
    else:
        for m in range(slabs):
            ks = list(range(m * slab_chips, (m + 1) * slab_chips))
            base = flip(chip // slab_chips, m)
            steps.append((ks[m == 0 :], ks, [(base * slab_chips * 2, 2 * slab_chips, base * slab, slab)]))

    for m, (coming, there, pieces) in enumerate(steps):
        forward(COLUMNS, col_buf, passed, coming, near)
        arrive(passed, there)
        ready = [piece_of(*piece) for piece in pieces]
        power = sum(piece[2] for piece in ready)
        scaled = jnp.concatenate([piece[1] for piece in ready], axis=1)
        if m:
            power = power + squares[...]
        last = m + 1 == len(steps)
        if last:
            scale = lax.rsqrt(power / width + epsilon)
        else:
            squares[...] = power
        for j in range(hidden // tile):
            span = slice(j * tile, (j + 1) * tile)
            g_rows = jnp.concatenate([wg[piece[0], span] for piece in ready], axis=0)
            u_rows = jnp.concatenate([wu[piece[0], span] for piece in ready], axis=0)
            g = jnp.dot(scaled, g_rows, preferred_element_type=F32)
            u = jnp.dot(scaled, u_rows, preferred_element_type=F32)
            if m:
                g = g + acc_gate[:, span]
                u = u + acc_up[:, span]
            if last:
                hid[:, span] = (jax.nn.silu(g * scale) * (u * scale)).astype(BF16)
            else:
                acc_gate[:, span] = g
                acc_up[:, span] = u
        if m == 0:
            update(2)
    loads[9].wait()
    out_tile = 256
    counts = [2]*(width//(2*out_tile))
    bounds = [sum(counts[:p]) * out_tile for p in range(len(counts) + 1)]

    halves = []

    def settle(p):
        part = pl.ds(bounds[p], bounds[p + 1] - bounds[p])
        halves[p].wait_recv()
        for c in range(chips):
            summed[c, :, part] = (
                ps[1 - core, c, :, part].astype(F32) + fw[c, :, part].astype(F32)
            ).astype(BF16)
        for k in far_first + [0]:
            send(
                RETURN, k, summed.at[at[k], :, part], ret_buf.at[chip, :, part], cross[k]
            )

    for p in range(len(counts)):
        for q in range(counts[p]):
            part = slice(bounds[p] + q * out_tile, bounds[p] + (q + 1) * out_tile)
            d = jnp.dot(hid[...], wd[:, part], preferred_element_type=F32)
            for s in range(n):
                ps[s % 2, s // 2, :, part] = d[s * rows : (s + 1) * rows, :].astype(BF16)
        part = pl.ds(bounds[p], bounds[p + 1] - bounds[p])
        halves.append(send(PAIR, p, ps.at[core, :, :, part], fw.at[:, :, part], partner))
        if p >= 2:
            settle(p - 2)
    for p in range(len(counts) - 2, len(counts)):
        settle(p)
    update(3)
    for phase, buf in ((MOVE, pj_send), (MIXED, mx_buf), (COLUMNS, col_buf)):
        whole(phase, 0, buf.at[pl.ds(0, n - 1)]).wait_send()
    whole(PAIR, 0, ps.at[0]).wait_send()

    @pl.when(late)
    def _():
        whole(GATHER, 0, tok_buf.at[pl.ds(0, chips)]).wait_send()

    @pl.when(jnp.logical_not(late))
    def _():
        whole(GATHER, 0, tok_buf).wait_send()
    whole(RETURN, 0, ret_buf).wait_recv()
    for load in loads[10:]:
        load.wait()
    own = mid_buf[chip]
    result = jnp.where(core == 0, own[:rows, :], own[rows:, :])
    diagonal = lax.broadcasted_iota(jnp.int32, (rows, rows), 0) == lax.broadcasted_iota(
        jnp.int32, (rows, rows), 1
    )
    for e in range(EXPERTS):
        flat_share = jnp.sum(
            jnp.where(ids[...] == e, weights[...].astype(F32), 0.0), axis=0, keepdims=True
        )
        share = jnp.sum(jnp.where(diagonal, flat_share, 0.0), axis=1, keepdims=True)
        rows_e = ret_buf[e * group].astype(F32)
        for s in range(1, group):
            rows_e = rows_e + ret_buf[e * group + s].astype(F32)
        result = result + share * rows_e
    layer_out[...] = result.astype(BF16)
    whole(RETURN, 0, summed).wait_send()


def write(layer_in, state_in, layer_out, state_out, sem):
    copies = [pltpu.make_async_copy(layer_in, layer_out, sem.at[0])]
    for t in range(state_in.shape[0]):
        copies.append(pltpu.make_async_copy(state_in.at[t], state_out.at[t], sem.at[1 + t]))
    for copy in copies:
        copy.start()
    for copy in copies:
        copy.wait()


def local(n, *args):
    (
        tokens,
        state,
        ids,
        weights,
        norm_mix,
        w_query,
        w_forget,
        w_input,
        w_gate,
        lower_bound,
        head_gain,
        w_out,
        norm_ffn,
        expert_gate,
        expert_up,
        expert_down,
    ) = args
    rows, width = tokens.shape
    heads, dim = state.shape[1], state.shape[2]
    cols = w_query.shape[1]
    hidden = expert_gate.shape[1]
    total = n * rows
    any_spec = pl.BlockSpec(memory_space=pltpu.HBM)
    vmem = pl.BlockSpec(memory_space=pltpu.VMEM)
    layer, fresh = pl.pallas_call(
        functools.partial(kernel, n),
        out_shape=(
            pltpu.VMEM(tokens.shape, tokens.dtype),
            pltpu.VMEM(state.shape, state.dtype),
        ),
        in_specs=[any_spec] * 16,
        out_specs=(vmem, vmem),
        scratch_shapes=[
            pltpu.VMEM((n, rows, width), BF16),
            pltpu.VMEM((1, width), F32),
            pltpu.VMEM((heads, 1, dim), F32),
            pltpu.VMEM((1, dim), F32),
            pltpu.VMEM((1, width), F32),
            pltpu.VMEM((4, width, cols), BF16),
            pltpu.VMEM((width, cols), BF16),
            pltpu.VMEM((width, hidden), BF16),
            pltpu.VMEM((width, hidden), BF16),
            pltpu.VMEM((hidden, width), BF16),
            pltpu.VMEM((total, width), BF16),
            pltpu.VMEM((n, rows, 4 * cols), BF16),
            pltpu.VMEM((n, rows, 4 * cols), BF16),
            pltpu.VMEM((heads, 4 * rows, dim), F32),
            pltpu.VMEM((n, rows, width), BF16),
            pltpu.VMEM((n, n // 2, 2 * rows, cols), BF16),
            pltpu.VMEM((n // 2, 2 * rows, width), F32),
            pltpu.VMEM((total, 1), F32),
            pltpu.VMEM((total, hidden), F32),
            pltpu.VMEM((total, hidden), F32),
            pltpu.VMEM((total, hidden), BF16),
            pltpu.VMEM((2, n // 2, rows, width), BF16),
            pltpu.VMEM((n // 2, rows, width), BF16),
            pltpu.VMEM((n // 2, rows, width), BF16),
            pltpu.VMEM((n // 2, rows, width), BF16),
            pltpu.VMEM(ids.T.shape, ids.dtype),
            pltpu.VMEM(weights.T.shape, weights.dtype),
            pltpu.SemaphoreType.DMA((16,)),
            pltpu.SemaphoreType.DMA((6,)),
            pltpu.SemaphoreType.DMA((2 * n + n // 2 + 1,)),
            pltpu.SemaphoreType.REGULAR,
        ],
        compiler_params=pltpu.CompilerParams(
            collective_id=0,
            has_side_effects=True,
            vmem_limit_bytes=VMEM - 4 * state.size - 64 * 1024,
        ),
    )(
        tokens,
        state,
        ids.T,
        weights.T,
        norm_mix[None],
        w_query,
        w_forget,
        w_input,
        w_gate,
        lower_bound.reshape(heads, 1, dim),
        head_gain[None],
        w_out,
        norm_ffn[None],
        expert_gate,
        expert_up,
        expert_down,
    )
    return pl.pallas_call(
        write,
        out_shape=(
            jax.ShapeDtypeStruct(layer.shape, layer.dtype),
            jax.ShapeDtypeStruct(fresh.shape, fresh.dtype),
        ),
        in_specs=[vmem, vmem],
        out_specs=(any_spec, any_spec),
        scratch_shapes=[pltpu.SemaphoreType.DMA((1 + rows,))],
        compiler_params=pltpu.CompilerParams(vmem_limit_bytes=1 << 20),
    )(
        pltpu.with_memory_space_constraint(layer, pltpu.VMEM),
        pltpu.with_memory_space_constraint(fresh, pltpu.VMEM),
    )


def solution(mesh):
    return jax.shard_map(
        functools.partial(local, mesh.shape["ep"]),
        mesh=mesh,
        in_specs=(
            P(("grp", "ep"), None),
            P(("grp", "ep"), None, None, None),
            P(("grp", "ep"), None),
            P(("grp", "ep"), None),
            P(),
            P(None, "ep"),
            P(None, "ep"),
            P(None, "ep"),
            P(None, "ep"),
            P(),
            P(),
            P(None, "ep"),
            P(),
            P(None, "ep"),
            P(None, "ep"),
            P("ep", None),
        ),
        out_specs=(P(("grp", "ep"), None), P(("grp", "ep"), None, None, None)),
        check_vma=False,
    )
```

```python
import functools

import jax
import jax.numpy as jnp
from jax import lax
from jax.experimental import pallas as pl
from jax.experimental.pallas import tpu as pltpu
from jax.sharding import PartitionSpec as P

FF = 7168
EXPERTS = 4
VMEM = 67043328

epsilon = 1e-06
F32 = jnp.float32
BF16 = jnp.bfloat16


def rms_scale(values, gain):
    return values * lax.rsqrt(jnp.mean(values * values, axis=-1, keepdims=True) + epsilon) * gain


def kernel(
    n,
    tokens,
    state,
    ids_in,
    weights_in,
    norm_mix_in,
    w_query,
    w_forget,
    w_input,
    w_gate,
    lower_bound_in,
    head_gain_in,
    w_out,
    norm_ffn_in,
    expert_gate,
    expert_up,
    expert_down,
    layer_out,
    st,
    tok_buf,
    norm_mix,
    lower_bound,
    head_gain,
    norm_ffn,
    wp,
    wo,
    wg,
    wu,
    wd,
    xn,
    pj_send,
    pj_buf,
    gates,
    mx_buf,
    col_buf,
    mid_buf,
    squares,
    acc_gate,
    acc_up,
    hid,
    ps,
    fw,
    summed,
    ret_buf,
    ids,
    weights,
    load_sem,
    send_sem,
    recv_sem,
    late_sem,
):
    me = lax.axis_index("ep")
    rows, width = tokens.shape
    heads, dim = state.shape[1], state.shape[2]
    cols = w_query.shape[1]
    total = n * rows
    hidden = expert_gate.shape[1]
    group = n // EXPERTS // 2
    both = 2 * rows

    loads = [pltpu.make_async_copy(tokens, tok_buf.at[me], load_sem.at[0])]
    for j, w in enumerate((w_query, w_forget, w_input, w_gate)):
        loads.append(pltpu.make_async_copy(w, wp.at[j], load_sem.at[1 + j]))
    loads.append(pltpu.make_async_copy(state, st, load_sem.at[5]))
    loads.append(pltpu.make_async_copy(w_out, wo, load_sem.at[6]))
    loads.append(pltpu.make_async_copy(expert_gate, wg, load_sem.at[7]))
    loads.append(pltpu.make_async_copy(expert_up, wu, load_sem.at[8]))
    loads.append(pltpu.make_async_copy(expert_down, wd, load_sem.at[9]))
    loads.append(pltpu.make_async_copy(ids_in, ids, load_sem.at[14]))
    loads.append(pltpu.make_async_copy(weights_in, weights, load_sem.at[15]))
    small = [
        pltpu.make_async_copy(a, b, load_sem.at[10 + j])
        for j, (a, b) in enumerate(
            (
                (norm_mix_in, norm_mix),
                (lower_bound_in, lower_bound),
                (head_gain_in, head_gain),
                (norm_ffn_in, norm_ffn),
            )
        )
    ]

    core = lax.rem(me, 2)
    chip = me // 2
    chips = n // 2
    partner = me + 1 - 2 * core

    def flip(index, k):
        bit = 1
        while bit <= k:
            if k & bit:
                index = index + bit * (1 - 2 * lax.rem(index // bit, 2))
            bit *= 2
        return index

    bits = [1 << b for b in range(chips.bit_length() - 1)]
    at = [flip(chip, k) for k in range(chips)]
    same = [2 * at[k] + core for k in range(chips)]
    cross = [2 * at[k] + 1 - core for k in range(chips)]
    far_first = list(range(chips - 1, 0, -1))
    barrier = pltpu.get_barrier_semaphore()
    late = chip == chips - 1

    def signal(semaphore, peer):
        pl.semaphore_signal(
            semaphore, inc=1, device_id={"ep": peer}, device_id_type=pl.DeviceIdType.MESH
        )

    @pl.when(late)
    def _():
        signal(barrier, partner)

    @pl.when(jnp.logical_not(late))
    def _():
        for k in far_first:
            signal(barrier, same[k])
            signal(barrier, cross[k])
        signal(barrier, partner)

    loads[0].start()

    @pl.when(late)
    def _():
        pl.semaphore_wait(barrier, n - 1)
        for k in far_first:
            signal(late_sem, same[k])
            signal(late_sem, cross[k])

    for load in small + loads[1:]:
        load.start()

    @pl.when(jnp.logical_not(late))
    def _():
        pl.semaphore_wait(barrier, n - 3)

    GATHER, MOVE, MIXED, COLUMNS, PAIR, RETURN = range(6)

    second, third = chips + chips // 2, 2 * chips + 1

    def lane(phase, slot, direct):
        if phase == MOVE:
            return second + slot // 4
        if phase == PAIR or (phase == MIXED and direct and slot):
            return third + slot
        if phase == RETURN:
            return third + chips
        if phase == COLUMNS and not direct:
            if slot == chips + 1:
                return second + chips // 2
            return second + (slot - chips) // 2 if slot else second
        return slot if direct else chips + (slot - chips) // 2

    def handle(phase, slot, source, target, peer, direct=False):
        return pltpu.make_async_remote_copy(
            src_ref=source,
            dst_ref=target,
            send_sem=send_sem.at[phase],
            recv_sem=recv_sem.at[lane(phase, slot, direct)],
            device_id={"ep": peer},
            device_id_type=pl.DeviceIdType.MESH,
        )

    def send(phase, slot, source, target, peer, direct=False):
        copy = handle(phase, slot, source, target, peer, direct)
        copy.start()
        return copy

    def whole(phase, slot, block, direct=False):
        return handle(phase, slot, block, block, partner, direct)

    def scatter(phase, block, near=0):
        for k in far_first:
            send(phase, k, block, block, cross[k], True)
            if k <= near:
                send(phase, chips + k, block, block, same[k])

    def forward(phase, buf, ks, near=0):
        for k in ks:
            if k == 0:
                send(phase, 0, buf.at[me], buf.at[me], partner, phase != COLUMNS)
            else:
                block = buf.at[cross[k]]
                whole(phase, k, block, True).wait_recv()
                if k > near:
                    send(phase, chips + k, block, block, partner)
                else:
                    whole(phase, chips + k, buf.at[same[k]]).wait_recv()

    def arrive(phase, buf, ks, near=0):
        for k in ks[::2]:
            if k:
                whole(phase, chips + k, buf.at[pl.ds(0, 2)]).wait_recv()
            else:
                whole(phase, 0, buf.at[0], phase != COLUMNS).wait_recv()
                if near < 1:
                    whole(phase, chips + 1, buf.at[0]).wait_recv()

    shares = [(chips * i // 4, chips * (i + 1) // 4) for i in range(4)]

    def base_of(index, lo, hi):
        return flip(index // (hi - lo), lo // (hi - lo)) * (hi - lo)

    def chip_rows(buf, k):
        return [buf[2 * at[k] + c].astype(F32) for c in range(2)]
    loads[0].wait()
    own = tok_buf.at[me]
    to_late = sum(bit * (1 - lax.rem(chip // bit, 2)) for bit in bits)
    direct = [handle(GATHER, k, own, own, cross[k] if k else partner, True) for k in range(chips)]
    extra = pltpu.make_async_remote_copy(
        src_ref=own,
        dst_ref=own,
        send_sem=send_sem.at[GATHER],
        recv_sem=recv_sem.at[chips + to_late // 2],
        device_id={"ep": n - 2 + core},
        device_id_type=pl.DeviceIdType.MESH,
    )
    for k in far_first:

        @pl.when(at[k] != chips - 1)
        def _(k=k):
            direct[k].start()

    @pl.when(jnp.logical_not(late))
    def _():
        direct[0].start()
        pl.semaphore_wait(late_sem, 2)
        extra.start()

    handle(GATHER, to_late, own, own, n - 1 - core, True).start()

    for load in small:
        load.wait()
    pairs = [[2 * j, 2 * j + 1] for j in range(chips // 2)]

    def norm_pair(j):
        x = jnp.concatenate([tok_buf[4 * j + i].astype(F32) for i in range(4)], axis=0)
        for i in range(2):
            mid_buf[2 * j + i] = x[i * both : (i + 1) * both, :]
        span = pl.ds(pl.multiple_of(2 * j * both, 2 * both), 2 * both)
        xn[span, :] = rms_scale(x, norm_mix[...]).astype(BF16)

    def relation(index):
        return sum(bit * lax.rem(chip // bit + index // bit, 2) for bit in bits)

    def pass_on(index):
        slot = relation(index)
        whole(GATHER, slot, own, True).wait_recv()

        @pl.when(jnp.logical_not(late))
        def _():
            block = tok_buf.at[2 * index + 1 - core]
            send(GATHER, chips + slot, block, block, partner)

    def settle_pair(j, first):
        if first:
            whole(GATHER, chips + 1, own).wait_recv()
        else:
            whole(GATHER, chips + relation(2 * j), tok_buf.at[pl.ds(0, 2)]).wait_recv()
        norm_pair(j)

    plane, planes = chip // 2, chips // 2
    order = [plane]
    for i in range(planes - 1):
        above = (i < planes - 1 - plane).astype(jnp.int32)
        order.append(above * (plane + 1 + i) + (1 - above) * (planes - 2 - i))
    whole(GATHER, 0, own, True).wait_recv()
    pass_on(at[1])
    for i in range(1, planes):
        pass_on(2 * order[i])
        pass_on(2 * order[i] + 1)
        settle_pair(order[i - 1], i == 1)
    settle_pair(order[-1], planes == 1)
    for load in loads[1:5]:
        load.wait()
    w_all = jnp.concatenate([wp[j] for j in range(4)], axis=1)
    acc = jnp.dot(xn[...], w_all, preferred_element_type=F32)
    for s in range(n):
        pj_send[s] = acc[s * rows : (s + 1) * rows, :].astype(BF16)
    for k in far_first + [0]:
        for r, peer in enumerate((same[k], cross[k])):
            if k or r:
                send(MOVE, 2 * k + r, pj_send.at[peer], pj_buf.at[me], peer)
    pj_buf[me] = pj_send[me]
    per_head = max(1, dim // cols)
    head_chips = max(1, per_head // 2)
    chip_heads = head_chips * 2 * cols // dim
    loads[5].wait()

    def head_step(h, first):
        def owned(j):
            return jnp.concatenate(
                [
                    pj_buf[first + i][:, j * cols : (j + 1) * cols].astype(F32)
                    for i in range(per_head)
                ],
                axis=1,
            )

        bound = lower_bound[h]
        forget_raw = owned(1)
        decay = bound + (1.0 - bound) * jax.nn.sigmoid(forget_raw)
        key_vec = (1.0 - bound) * jax.nn.sigmoid(-forget_raw)
        query_vec = jax.nn.silu(owned(0)) * dim ** (-0.5)
        input_raw = owned(2)
        read_vec = query_vec * decay
        gates[h] = jnp.concatenate([read_vec, decay, key_vec, input_raw], axis=0)
        wide = jnp.dot(
            read_vec,
            jnp.concatenate([st[t, h] for t in range(rows)], axis=1),
            preferred_element_type=F32,
        )
        read = jnp.concatenate(
            [wide[t : t + 1, t * dim : (t + 1) * dim] for t in range(rows)], axis=0
        ) + input_raw * jnp.sum(query_vec * key_vec, axis=1, keepdims=True)
        mixed = rms_scale(read, head_gain[...]) * jax.nn.silu(owned(3))
        part = pl.ds(pl.multiple_of(h * dim, dim), dim)
        mx_buf[me, :, part] = mixed.astype(BF16)

    for lo, hi in shares:
        step = max(2, head_chips)
        for first in range(lo, hi, step):
            for k in range(first, first + step, 2):
                count = 4 if k else 3
                whole(MOVE, 2 * k, pj_buf.at[pl.ds(0, count)]).wait_recv()
            for m in range(first // head_chips, (first + step) // head_chips):
                base = flip(chip // head_chips, m)
                for i in range(chip_heads):
                    head_step(base * chip_heads + i, base * head_chips * 2 + i * per_head)
        size = (hi - lo) * 2 * cols
        offset = pl.multiple_of(base_of(chip, lo, hi) * 2 * cols, size)
        scatter(MIXED, mx_buf.at[me, :, pl.ds(offset, size)])

    def update_step(h, carry):
        flat = gates[h]
        turned = flat.T
        for t in range(rows):
            st[t, h] = (
                turned[:, rows + t : rows + t + 1] * st[t, h]
                + turned[:, 2 * rows + t : 2 * rows + t + 1]
                * flat[3 * rows + t : 3 * rows + t + 1, :]
            )
        return carry

    cuts = [heads * c // 16 for c in (0, 8, 11, 13, 16)]

    def update(c):
        lax.fori_loop(cuts[c], cuts[c + 1], update_step, 0, unroll=2)
    forward(MIXED, mx_buf, [0])
    loads[6].wait()
    update(0)
    near = min(1, chips - 1)

    def gather_pair(ks):
        arrive(MIXED, mx_buf, ks)
        x = jnp.concatenate([part for k in ks for part in chip_rows(mx_buf, k)], axis=0)
        xn[ks[0] * both : (ks[0] + 2) * both, :] = x.astype(BF16)

    def project(lo, hi):
        acc = jnp.dot(xn[lo * both : hi * both, :], wo[...], preferred_element_type=F32)
        for k in range(lo, hi):
            col_buf[me, at[k]] = acc[(k - lo) * both : (k - lo + 1) * both, :].astype(BF16)
        base = base_of(chip, lo, hi)
        scatter(COLUMNS, col_buf.at[me, pl.ds(base, hi - lo)], near)

    for j, ks in enumerate(pairs):
        forward(MIXED, mx_buf, [k for k in ks if k])
        if j:
            gather_pair(pairs[j - 1])
            ready = 2 * j
            if ready == chips // 4:
                project(0, ready)
            if ready == chips // 2:
                project(chips // 4, ready)
    gather_pair(pairs[-1])
    project(chips // 2, chips)
    forward(COLUMNS, col_buf, [0])
    update(1)
    loads[7].wait()
    loads[8].wait()
    tile = 256 if hidden % 256 == 0 else hidden
    slab_chips = max(1, 256 // (2 * cols))
    slab = slab_chips * 2 * cols
    slabs = chips // slab_chips

    def piece_of(first, count, offset, size):
        part = pl.ds(pl.multiple_of(offset, size), size)
        y = jnp.concatenate([col_buf[first + i].astype(F32) for i in range(count)], axis=2)
        middle = mid_buf[:, :, part] + y
        mid_buf[:, :, part] = middle
        scaled = (middle * norm_ffn[:, part]).reshape(total, size).astype(BF16)
        return part, scaled, jnp.sum((middle * middle).reshape(total, size), axis=1, keepdims=True)

    steps = []
    if cols % 128 == 0:

        def devices(peers):
            return [(peer, 1, peer * cols, cols) for peer in peers]

        steps.append(([], [0], [(2 * chip, 2, chip * slab, slab)]))
        if near:
            steps.append(([1], [], [(2 * at[1], 2, at[1] * slab, slab)]))
        rest = [[k, k + 1] for k in range(2 * near, chips, 2)]
        for ks in rest:
            steps.append((ks, [], devices(cross[k] for k in ks)))
        for ks in rest:
            steps.append(([], ks, devices(same[k] for k in ks)))
    else:
        for m in range(slabs):
            ks = list(range(m * slab_chips, (m + 1) * slab_chips))
            base = flip(chip // slab_chips, m)
            steps.append((ks[m == 0 :], ks, [(base * slab_chips * 2, 2 * slab_chips, base * slab, slab)]))

    for m, (coming, there, pieces) in enumerate(steps):
        forward(COLUMNS, col_buf, coming, near)
        arrive(COLUMNS, col_buf, there, near)
        ready = [piece_of(*piece) for piece in pieces]
        power = sum(piece[2] for piece in ready)
        scaled = jnp.concatenate([piece[1] for piece in ready], axis=1)
        if m:
            power = power + squares[...]
        last = m + 1 == len(steps)
        if last:
            scale = lax.rsqrt(power / width + epsilon)
        else:
            squares[...] = power
        for j in range(hidden // tile):
            span = slice(j * tile, (j + 1) * tile)
            g_rows = jnp.concatenate([wg[piece[0], span] for piece in ready], axis=0)
            u_rows = jnp.concatenate([wu[piece[0], span] for piece in ready], axis=0)
            g = jnp.dot(scaled, g_rows, preferred_element_type=F32)
            u = jnp.dot(scaled, u_rows, preferred_element_type=F32)
            if m:
                g = g + acc_gate[:, span]
                u = u + acc_up[:, span]
            if last:
                hid[:, span] = (jax.nn.silu(g * scale) * (u * scale)).astype(BF16)
            else:
                acc_gate[:, span] = g
                acc_up[:, span] = u
        if m == 0:
            update(2)
    loads[9].wait()
    out_tile = 256
    counts = [2]*(width//(2*out_tile))
    bounds = [sum(counts[:p]) * out_tile for p in range(len(counts) + 1)]

    halves = []

    def settle(p):
        part = pl.ds(bounds[p], bounds[p + 1] - bounds[p])
        halves[p].wait_recv()
        for c in range(chips):
            summed[c, :, part] = (
                ps[1 - core, c, :, part].astype(F32) + fw[c, :, part].astype(F32)
            ).astype(BF16)
        for k in far_first + [0]:
            send(
                RETURN, k, summed.at[at[k], :, part], ret_buf.at[chip, :, part], cross[k]
            )

    for p in range(len(counts)):
        for q in range(counts[p]):
            part = slice(bounds[p] + q * out_tile, bounds[p] + (q + 1) * out_tile)
            d = jnp.dot(hid[...], wd[:, part], preferred_element_type=F32)
            for s in range(n):
                ps[s % 2, s // 2, :, part] = d[s * rows : (s + 1) * rows, :].astype(BF16)
        part = pl.ds(bounds[p], bounds[p + 1] - bounds[p])
        halves.append(send(PAIR, p, ps.at[core, :, :, part], fw.at[:, :, part], partner))
        if p >= 2:
            settle(p - 2)
    for p in range(len(counts) - 2, len(counts)):
        settle(p)
    update(3)
    for phase, buf in ((MOVE, pj_send), (MIXED, mx_buf), (COLUMNS, col_buf)):
        whole(phase, 0, buf.at[pl.ds(0, n - 1)]).wait_send()
    whole(PAIR, 0, ps.at[0]).wait_send()

    @pl.when(late)
    def _():
        whole(GATHER, 0, tok_buf.at[pl.ds(0, chips)]).wait_send()

    @pl.when(jnp.logical_not(late))
    def _():
        whole(GATHER, 0, tok_buf).wait_send()
    whole(RETURN, 0, ret_buf).wait_recv()
    for load in loads[10:]:
        load.wait()
    own = mid_buf[chip]
    result = jnp.where(core == 0, own[:rows, :], own[rows:, :])
    diagonal = lax.broadcasted_iota(jnp.int32, (rows, rows), 0) == lax.broadcasted_iota(
        jnp.int32, (rows, rows), 1
    )
    for e in range(EXPERTS):
        flat_share = jnp.sum(
            jnp.where(ids[...] == e, weights[...].astype(F32), 0.0), axis=0, keepdims=True
        )
        share = jnp.sum(jnp.where(diagonal, flat_share, 0.0), axis=1, keepdims=True)
        rows_e = ret_buf[e * group].astype(F32)
        for s in range(1, group):
            rows_e = rows_e + ret_buf[e * group + s].astype(F32)
        result = result + share * rows_e
    layer_out[...] = result.astype(BF16)
    whole(RETURN, 0, summed).wait_send()


def write(layer_in, state_in, layer_out, state_out, sem):
    copies = [pltpu.make_async_copy(layer_in, layer_out, sem.at[0])]
    for t in range(state_in.shape[0]):
        copies.append(pltpu.make_async_copy(state_in.at[t], state_out.at[t], sem.at[1 + t]))
    for copy in copies:
        copy.start()
    for copy in copies:
        copy.wait()


def local(n, *args):
    (
        tokens,
        state,
        ids,
        weights,
        norm_mix,
        w_query,
        w_forget,
        w_input,
        w_gate,
        lower_bound,
        head_gain,
        w_out,
        norm_ffn,
        expert_gate,
        expert_up,
        expert_down,
    ) = args
    rows, width = tokens.shape
    heads, dim = state.shape[1], state.shape[2]
    cols = w_query.shape[1]
    hidden = expert_gate.shape[1]
    total = n * rows
    any_spec = pl.BlockSpec(memory_space=pltpu.HBM)
    vmem = pl.BlockSpec(memory_space=pltpu.VMEM)
    layer, fresh = pl.pallas_call(
        functools.partial(kernel, n),
        out_shape=(
            pltpu.VMEM(tokens.shape, tokens.dtype),
            pltpu.VMEM(state.shape, state.dtype),
        ),
        in_specs=[any_spec] * 16,
        out_specs=(vmem, vmem),
        scratch_shapes=[
            pltpu.VMEM((n, rows, width), BF16),
            pltpu.VMEM((1, width), F32),
            pltpu.VMEM((heads, 1, dim), F32),
            pltpu.VMEM((1, dim), F32),
            pltpu.VMEM((1, width), F32),
            pltpu.VMEM((4, width, cols), BF16),
            pltpu.VMEM((width, cols), BF16),
            pltpu.VMEM((width, hidden), BF16),
            pltpu.VMEM((width, hidden), BF16),
            pltpu.VMEM((hidden, width), BF16),
            pltpu.VMEM((total, width), BF16),
            pltpu.VMEM((n, rows, 4 * cols), BF16),
            pltpu.VMEM((n, rows, 4 * cols), BF16),
            pltpu.VMEM((heads, 4 * rows, dim), F32),
            pltpu.VMEM((n, rows, width), BF16),
            pltpu.VMEM((n, n // 2, 2 * rows, cols), BF16),
            pltpu.VMEM((n // 2, 2 * rows, width), F32),
            pltpu.VMEM((total, 1), F32),
            pltpu.VMEM((total, hidden), F32),
            pltpu.VMEM((total, hidden), F32),
            pltpu.VMEM((total, hidden), BF16),
            pltpu.VMEM((2, n // 2, rows, width), BF16),
            pltpu.VMEM((n // 2, rows, width), BF16),
            pltpu.VMEM((n // 2, rows, width), BF16),
            pltpu.VMEM((n // 2, rows, width), BF16),
            pltpu.VMEM(ids.T.shape, ids.dtype),
            pltpu.VMEM(weights.T.shape, weights.dtype),
            pltpu.SemaphoreType.DMA((16,)),
            pltpu.SemaphoreType.DMA((6,)),
            pltpu.SemaphoreType.DMA((3 * (n // 2) + 2,)),
            pltpu.SemaphoreType.REGULAR,
        ],
        compiler_params=pltpu.CompilerParams(
            collective_id=0,
            has_side_effects=True,
            vmem_limit_bytes=VMEM - 4 * state.size - 64 * 1024,
        ),
    )(
        tokens,
        state,
        ids.T,
        weights.T,
        norm_mix[None],
        w_query,
        w_forget,
        w_input,
        w_gate,
        lower_bound.reshape(heads, 1, dim),
        head_gain[None],
        w_out,
        norm_ffn[None],
        expert_gate,
        expert_up,
        expert_down,
    )
    return pl.pallas_call(
        write,
        out_shape=(
            jax.ShapeDtypeStruct(layer.shape, layer.dtype),
            jax.ShapeDtypeStruct(fresh.shape, fresh.dtype),
        ),
        in_specs=[vmem, vmem],
        out_specs=(any_spec, any_spec),
        scratch_shapes=[pltpu.SemaphoreType.DMA((1 + rows,))],
        compiler_params=pltpu.CompilerParams(vmem_limit_bytes=1 << 20),
    )(
        pltpu.with_memory_space_constraint(layer, pltpu.VMEM),
        pltpu.with_memory_space_constraint(fresh, pltpu.VMEM),
    )


def solution(mesh):
    return jax.shard_map(
        functools.partial(local, mesh.shape["ep"]),
        mesh=mesh,
        in_specs=(
            P(("grp", "ep"), None),
            P(("grp", "ep"), None, None, None),
            P(("grp", "ep"), None),
            P(("grp", "ep"), None),
            P(),
            P(None, "ep"),
            P(None, "ep"),
            P(None, "ep"),
            P(None, "ep"),
            P(),
            P(),
            P(None, "ep"),
            P(),
            P(None, "ep"),
            P(None, "ep"),
            P("ep", None),
        ),
        out_specs=(P(("grp", "ep"), None), P(("grp", "ep"), None, None, None)),
        check_vma=False,
    )
```

```python
import functools

import jax
import jax.numpy as jnp
from jax import lax
from jax.experimental import pallas as pl
from jax.experimental.pallas import tpu as pltpu
from jax.sharding import PartitionSpec as P

FF = 7168
EXPERTS = 4
VMEM = 67043328

epsilon = 1e-06
F32 = jnp.float32
BF16 = jnp.bfloat16


def rms_scale(values, gain):
    return values * lax.rsqrt(jnp.mean(values * values, axis=-1, keepdims=True) + epsilon) * gain


def kernel(
    n,
    tokens,
    state,
    ids_in,
    weights_in,
    norm_mix_in,
    w_query,
    w_forget,
    w_input,
    w_gate,
    lower_bound_in,
    head_gain_in,
    w_out,
    norm_ffn_in,
    expert_gate,
    expert_up,
    expert_down,
    layer_out,
    st,
    tok_buf,
    norm_mix,
    lower_bound,
    head_gain,
    norm_ffn,
    wp,
    wo,
    wg,
    wu,
    wd,
    xn,
    pj_send,
    pj_buf,
    gates,
    mx_buf,
    col_buf,
    mid_buf,
    squares,
    acc_gate,
    acc_up,
    hid,
    ps,
    fw,
    summed,
    ret_buf,
    ids,
    weights,
    load_sem,
    send_sem,
    recv_sem,
    late_sem,
):
    me = lax.axis_index("ep")
    rows, width = tokens.shape
    heads, dim = state.shape[1], state.shape[2]
    cols = w_query.shape[1]
    total = n * rows
    hidden = expert_gate.shape[1]
    group = n // EXPERTS // 2
    both = 2 * rows

    loads = [pltpu.make_async_copy(tokens, tok_buf.at[me], load_sem.at[0])]
    for j, w in enumerate((w_query, w_forget, w_input, w_gate)):
        loads.append(pltpu.make_async_copy(w, wp.at[j], load_sem.at[1 + j]))
    loads.append(pltpu.make_async_copy(state, st, load_sem.at[5]))
    loads.append(pltpu.make_async_copy(w_out, wo, load_sem.at[6]))
    loads.append(pltpu.make_async_copy(expert_gate, wg, load_sem.at[7]))
    loads.append(pltpu.make_async_copy(expert_up, wu, load_sem.at[8]))
    loads.append(pltpu.make_async_copy(expert_down, wd, load_sem.at[9]))
    loads.append(pltpu.make_async_copy(ids_in, ids, load_sem.at[14]))
    loads.append(pltpu.make_async_copy(weights_in, weights, load_sem.at[15]))
    small = [
        pltpu.make_async_copy(a, b, load_sem.at[10 + j])
        for j, (a, b) in enumerate(
            (
                (norm_mix_in, norm_mix),
                (lower_bound_in, lower_bound),
                (head_gain_in, head_gain),
                (norm_ffn_in, norm_ffn),
            )
        )
    ]

    core = lax.rem(me, 2)
    chip = me // 2
    chips = n // 2
    partner = me + 1 - 2 * core

    def flip(index, k):
        bit = 1
        while bit <= k:
            if k & bit:
                index = index + bit * (1 - 2 * lax.rem(index // bit, 2))
            bit *= 2
        return index

    bits = [1 << b for b in range(chips.bit_length() - 1)]
    at = [flip(chip, k) for k in range(chips)]
    same = [2 * at[k] + core for k in range(chips)]
    cross = [2 * at[k] + 1 - core for k in range(chips)]
    far_first = list(range(chips - 1, 0, -1))
    barrier = pltpu.get_barrier_semaphore()
    late = chip == chips - 1

    def signal(semaphore, peer):
        pl.semaphore_signal(
            semaphore, inc=1, device_id={"ep": peer}, device_id_type=pl.DeviceIdType.MESH
        )

    @pl.when(late)
    def _():
        signal(barrier, partner)

    @pl.when(jnp.logical_not(late))
    def _():
        for k in far_first:
            signal(barrier, same[k])
            signal(barrier, cross[k])
        signal(barrier, partner)

    loads[0].start()

    @pl.when(late)
    def _():
        pl.semaphore_wait(barrier, n - 1)
        for k in far_first:
            signal(late_sem, same[k])
            signal(late_sem, cross[k])

    for load in small:
        load.start()

    @pl.when(jnp.logical_not(late))
    def _():
        for load in loads[1:]:
            load.start()
        pl.semaphore_wait(barrier, n - 3)

    GATHER, MOVE, MIXED, COLUMNS, PAIR, RETURN = range(6)

    second, third = chips + chips // 2, 2 * chips + 1

    def lane(phase, slot, direct):
        if phase == MOVE:
            return second + slot // 4
        if phase == PAIR or (phase == MIXED and direct and slot):
            return third + slot
        if phase == RETURN:
            return third + chips
        if phase == COLUMNS and not direct:
            if slot == chips + 1:
                return second + chips // 2
            return second + (slot - chips) // 2 if slot else second
        return slot if direct else chips + (slot - chips) // 2

    def handle(phase, slot, source, target, peer, direct=False):
        return pltpu.make_async_remote_copy(
            src_ref=source,
            dst_ref=target,
            send_sem=send_sem.at[phase],
            recv_sem=recv_sem.at[lane(phase, slot, direct)],
            device_id={"ep": peer},
            device_id_type=pl.DeviceIdType.MESH,
        )

    def send(phase, slot, source, target, peer, direct=False):
        copy = handle(phase, slot, source, target, peer, direct)
        copy.start()
        return copy

    def whole(phase, slot, block, direct=False):
        return handle(phase, slot, block, block, partner, direct)

    def scatter(phase, block, near=0):
        for k in far_first:
            send(phase, k, block, block, cross[k], True)
            if k <= near:
                send(phase, chips + k, block, block, same[k])

    def forward(phase, buf, ks, near=0):
        for k in ks:
            if k == 0:
                send(phase, 0, buf.at[me], buf.at[me], partner, phase != COLUMNS)
            else:
                block = buf.at[cross[k]]
                whole(phase, k, block, True).wait_recv()
                if k > near:
                    send(phase, chips + k, block, block, partner)
                else:
                    whole(phase, chips + k, buf.at[same[k]]).wait_recv()

    def arrive(phase, buf, ks, near=0):
        for k in ks[::2]:
            if k:
                whole(phase, chips + k, buf.at[pl.ds(0, 2)]).wait_recv()
            else:
                whole(phase, 0, buf.at[0], phase != COLUMNS).wait_recv()
                if near < 1:
                    whole(phase, chips + 1, buf.at[0]).wait_recv()

    shares = [(0, chips // 4), (chips // 4, chips // 2), (chips // 2, chips)]

    def base_of(index, lo, hi):
        return flip(index // (hi - lo), lo // (hi - lo)) * (hi - lo)

    def chip_rows(buf, k):
        return [buf[2 * at[k] + c].astype(F32) for c in range(2)]
    loads[0].wait()
    own = tok_buf.at[me]
    to_late = sum(bit * (1 - lax.rem(chip // bit, 2)) for bit in bits)
    direct = [handle(GATHER, k, own, own, cross[k] if k else partner, True) for k in range(chips)]
    extra = pltpu.make_async_remote_copy(
        src_ref=own,
        dst_ref=own,
        send_sem=send_sem.at[GATHER],
        recv_sem=recv_sem.at[chips + to_late // 2],
        device_id={"ep": n - 2 + core},
        device_id_type=pl.DeviceIdType.MESH,
    )
    for k in far_first:

        @pl.when(at[k] != chips - 1)
        def _(k=k):
            direct[k].start()

    @pl.when(jnp.logical_not(late))
    def _():
        direct[0].start()
        pl.semaphore_wait(late_sem, 2)
        extra.start()

    handle(GATHER, to_late, own, own, n - 1 - core, True).start()

    @pl.when(late)
    def _():
        for load in loads[1:]:
            load.start()

    for load in small:
        load.wait()
    pairs = [[2 * j, 2 * j + 1] for j in range(chips // 2)]

    def norm_pair(j):
        x = jnp.concatenate([tok_buf[4 * j + i].astype(F32) for i in range(4)], axis=0)
        for i in range(2):
            mid_buf[2 * j + i] = x[i * both : (i + 1) * both, :]
        span = pl.ds(pl.multiple_of(2 * j * both, 2 * both), 2 * both)
        xn[span, :] = rms_scale(x, norm_mix[...]).astype(BF16)

    def relation(index):
        return sum(bit * lax.rem(chip // bit + index // bit, 2) for bit in bits)

    def pass_on(index):
        slot = relation(index)
        whole(GATHER, slot, own, True).wait_recv()

        @pl.when(jnp.logical_not(late))
        def _():
            block = tok_buf.at[2 * index + 1 - core]
            send(GATHER, chips + slot, block, block, partner)

    def settle_pair(j, first):
        if first:
            whole(GATHER, chips + 1, own).wait_recv()
        else:
            whole(GATHER, chips + relation(2 * j), tok_buf.at[pl.ds(0, 2)]).wait_recv()
        norm_pair(j)

    plane, planes = chip // 2, chips // 2
    order = [plane]
    for i in range(planes - 1):
        above = (i < planes - 1 - plane).astype(jnp.int32)
        order.append(above * (plane + 1 + i) + (1 - above) * (planes - 2 - i))
    whole(GATHER, 0, own, True).wait_recv()
    pass_on(at[1])
    for i in range(1, planes):
        pass_on(2 * order[i])
        pass_on(2 * order[i] + 1)
        settle_pair(order[i - 1], i == 1)
    settle_pair(order[-1], planes == 1)
    for load in loads[1:5]:
        load.wait()
    w_all = jnp.concatenate([wp[j] for j in range(4)], axis=1)
    acc = jnp.dot(xn[...], w_all, preferred_element_type=F32)
    for s in range(n):
        pj_send[s] = acc[s * rows : (s + 1) * rows, :].astype(BF16)
    for k in far_first + [0]:
        for r, peer in enumerate((same[k], cross[k])):
            if k or r:
                send(MOVE, 2 * k + r, pj_send.at[peer], pj_buf.at[me], peer)
    pj_buf[me] = pj_send[me]
    per_head = max(1, dim // cols)
    head_chips = max(1, per_head // 2)
    chip_heads = head_chips * 2 * cols // dim
    loads[5].wait()

    def head_step(h, first):
        def owned(j):
            return jnp.concatenate(
                [
                    pj_buf[first + i][:, j * cols : (j + 1) * cols].astype(F32)
                    for i in range(per_head)
                ],
                axis=1,
            )

        bound = lower_bound[h]
        forget_raw = owned(1)
        decay = bound + (1.0 - bound) * jax.nn.sigmoid(forget_raw)
        key_vec = (1.0 - bound) * jax.nn.sigmoid(-forget_raw)
        query_vec = jax.nn.silu(owned(0)) * dim ** (-0.5)
        input_raw = owned(2)
        read_vec = query_vec * decay
        gates[h] = jnp.concatenate([read_vec, decay, key_vec, input_raw], axis=0)
        wide = jnp.dot(
            read_vec,
            jnp.concatenate([st[t, h] for t in range(rows)], axis=1),
            preferred_element_type=F32,
        )
        read = jnp.concatenate(
            [wide[t : t + 1, t * dim : (t + 1) * dim] for t in range(rows)], axis=0
        ) + input_raw * jnp.sum(query_vec * key_vec, axis=1, keepdims=True)
        mixed = rms_scale(read, head_gain[...]) * jax.nn.silu(owned(3))
        part = pl.ds(pl.multiple_of(h * dim, dim), dim)
        mx_buf[me, :, part] = mixed.astype(BF16)

    for lo, hi in shares:
        step = max(2, head_chips, hi - lo)
        for first in range(lo, hi, step):
            for k in range(first, first + step, 2):
                count = 4 if k else 3
                whole(MOVE, 2 * k, pj_buf.at[pl.ds(0, count)]).wait_recv()
            for m in range(first // head_chips, (first + step) // head_chips):
                base = flip(chip // head_chips, m)
                for i in range(chip_heads):
                    head_step(base * chip_heads + i, base * head_chips * 2 + i * per_head)
        size = (hi - lo) * 2 * cols
        offset = pl.multiple_of(base_of(chip, lo, hi) * 2 * cols, size)
        scatter(MIXED, mx_buf.at[me, :, pl.ds(offset, size)])

    def update_step(h, carry):
        flat = gates[h]
        turned = flat.T
        for t in range(rows):
            st[t, h] = (
                turned[:, rows + t : rows + t + 1] * st[t, h]
                + turned[:, 2 * rows + t : 2 * rows + t + 1]
                * flat[3 * rows + t : 3 * rows + t + 1, :]
            )
        return carry

    cuts = [heads * c // 16 for c in (0, 8, 11, 13, 16)]

    def update(c):
        lax.fori_loop(cuts[c], cuts[c + 1], update_step, 0, unroll=2)
    forward(MIXED, mx_buf, [0])
    loads[6].wait()
    update(0)
    near = min(1, chips - 1)

    def gather_pair(ks):
        arrive(MIXED, mx_buf, ks)
        x = jnp.concatenate([part for k in ks for part in chip_rows(mx_buf, k)], axis=0)
        xn[ks[0] * both : (ks[0] + 2) * both, :] = x.astype(BF16)

    def project(lo, hi):
        acc = jnp.dot(xn[lo * both : hi * both, :], wo[...], preferred_element_type=F32)
        for k in range(lo, hi):
            col_buf[me, at[k]] = acc[(k - lo) * both : (k - lo + 1) * both, :].astype(BF16)
        base = base_of(chip, lo, hi)
        scatter(COLUMNS, col_buf.at[me, pl.ds(base, hi - lo)], near)

    for j, ks in enumerate(pairs):
        forward(MIXED, mx_buf, [k for k in ks if k])
        if j:
            gather_pair(pairs[j - 1])
            ready = 2 * j
            if ready == chips // 4:
                project(0, ready)
            if ready == chips // 2:
                project(chips // 4, ready)
    gather_pair(pairs[-1])
    project(chips // 2, chips)
    forward(COLUMNS, col_buf, [0])
    update(1)
    loads[7].wait()
    loads[8].wait()
    tile = 256 if hidden % 256 == 0 else hidden
    slab_chips = max(1, 256 // (2 * cols))
    slab = slab_chips * 2 * cols
    slabs = chips // slab_chips

    def piece_of(first, count, offset, size):
        part = pl.ds(pl.multiple_of(offset, size), size)
        y = jnp.concatenate([col_buf[first + i].astype(F32) for i in range(count)], axis=2)
        middle = mid_buf[:, :, part] + y
        mid_buf[:, :, part] = middle
        scaled = (middle * norm_ffn[:, part]).reshape(total, size).astype(BF16)
        return part, scaled, jnp.sum((middle * middle).reshape(total, size), axis=1, keepdims=True)

    steps = []
    if cols % 128 == 0:

        def devices(peers):
            return [(peer, 1, peer * cols, cols) for peer in peers]

        steps.append(([], [0], [(2 * chip, 2, chip * slab, slab)]))
        if near:
            steps.append(([1], [], [(2 * at[1], 2, at[1] * slab, slab)]))
        rest = [[k, k + 1] for k in range(2 * near, chips, 2)]
        for ks in rest:
            steps.append((ks, [], devices(cross[k] for k in ks)))
        for ks in rest:
            steps.append(([], ks, devices(same[k] for k in ks)))
    else:
        for m in range(slabs):
            ks = list(range(m * slab_chips, (m + 1) * slab_chips))
            base = flip(chip // slab_chips, m)
            steps.append((ks[m == 0 :], ks, [(base * slab_chips * 2, 2 * slab_chips, base * slab, slab)]))

    for m, (coming, there, pieces) in enumerate(steps):
        forward(COLUMNS, col_buf, coming, near)
        arrive(COLUMNS, col_buf, there, near)
        ready = [piece_of(*piece) for piece in pieces]
        power = sum(piece[2] for piece in ready)
        scaled = jnp.concatenate([piece[1] for piece in ready], axis=1)
        if m:
            power = power + squares[...]
        last = m + 1 == len(steps)
        if last:
            scale = lax.rsqrt(power / width + epsilon)
        else:
            squares[...] = power
        for j in range(hidden // tile):
            span = slice(j * tile, (j + 1) * tile)
            g_rows = jnp.concatenate([wg[piece[0], span] for piece in ready], axis=0)
            u_rows = jnp.concatenate([wu[piece[0], span] for piece in ready], axis=0)
            g = jnp.dot(scaled, g_rows, preferred_element_type=F32)
            u = jnp.dot(scaled, u_rows, preferred_element_type=F32)
            if m:
                g = g + acc_gate[:, span]
                u = u + acc_up[:, span]
            if last:
                hid[:, span] = (jax.nn.silu(g * scale) * (u * scale)).astype(BF16)
            else:
                acc_gate[:, span] = g
                acc_up[:, span] = u
        if m == 0:
            update(2)
    loads[9].wait()
    out_tile = 256
    counts = [2]*(width//(2*out_tile))
    bounds = [sum(counts[:p]) * out_tile for p in range(len(counts) + 1)]

    halves = []

    def settle(p):
        part = pl.ds(bounds[p], bounds[p + 1] - bounds[p])
        halves[p].wait_recv()
        for c in range(chips):
            summed[c, :, part] = (
                ps[1 - core, c, :, part].astype(F32) + fw[c, :, part].astype(F32)
            ).astype(BF16)
        for k in far_first + [0]:
            send(
                RETURN, k, summed.at[at[k], :, part], ret_buf.at[chip, :, part], cross[k]
            )

    for p in range(len(counts)):
        for q in range(counts[p]):
            part = slice(bounds[p] + q * out_tile, bounds[p] + (q + 1) * out_tile)
            d = jnp.dot(hid[...], wd[:, part], preferred_element_type=F32)
            for s in range(n):
                ps[s % 2, s // 2, :, part] = d[s * rows : (s + 1) * rows, :].astype(BF16)
        part = pl.ds(bounds[p], bounds[p + 1] - bounds[p])
        halves.append(send(PAIR, p, ps.at[core, :, :, part], fw.at[:, :, part], partner))
        if p >= 2:
            settle(p - 2)
    for p in range(len(counts) - 2, len(counts)):
        settle(p)
    update(3)
    for phase, buf in ((MOVE, pj_send), (MIXED, mx_buf), (COLUMNS, col_buf)):
        whole(phase, 0, buf.at[pl.ds(0, n - 1)]).wait_send()
    whole(PAIR, 0, ps.at[0]).wait_send()

    @pl.when(late)
    def _():
        whole(GATHER, 0, tok_buf.at[pl.ds(0, chips)]).wait_send()

    @pl.when(jnp.logical_not(late))
    def _():
        whole(GATHER, 0, tok_buf).wait_send()
    whole(RETURN, 0, ret_buf).wait_recv()
    for load in loads[10:]:
        load.wait()
    own = mid_buf[chip]
    result = jnp.where(core == 0, own[:rows, :], own[rows:, :])
    diagonal = lax.broadcasted_iota(jnp.int32, (rows, rows), 0) == lax.broadcasted_iota(
        jnp.int32, (rows, rows), 1
    )
    for e in range(EXPERTS):
        flat_share = jnp.sum(
            jnp.where(ids[...] == e, weights[...].astype(F32), 0.0), axis=0, keepdims=True
        )
        share = jnp.sum(jnp.where(diagonal, flat_share, 0.0), axis=1, keepdims=True)
        rows_e = ret_buf[e * group].astype(F32)
        for s in range(1, group):
            rows_e = rows_e + ret_buf[e * group + s].astype(F32)
        result = result + share * rows_e
    layer_out[...] = result.astype(BF16)
    whole(RETURN, 0, summed).wait_send()


def write(layer_in, state_in, layer_out, state_out, sem):
    copies = [pltpu.make_async_copy(layer_in, layer_out, sem.at[0])]
    for t in range(state_in.shape[0]):
        copies.append(pltpu.make_async_copy(state_in.at[t], state_out.at[t], sem.at[1 + t]))
    for copy in copies:
        copy.start()
    for copy in copies:
        copy.wait()


def local(n, *args):
    (
        tokens,
        state,
        ids,
        weights,
        norm_mix,
        w_query,
        w_forget,
        w_input,
        w_gate,
        lower_bound,
        head_gain,
        w_out,
        norm_ffn,
        expert_gate,
        expert_up,
        expert_down,
    ) = args
    rows, width = tokens.shape
    heads, dim = state.shape[1], state.shape[2]
    cols = w_query.shape[1]
    hidden = expert_gate.shape[1]
    total = n * rows
    any_spec = pl.BlockSpec(memory_space=pltpu.HBM)
    vmem = pl.BlockSpec(memory_space=pltpu.VMEM)
    layer, fresh = pl.pallas_call(
        functools.partial(kernel, n),
        out_shape=(
            pltpu.VMEM(tokens.shape, tokens.dtype),
            pltpu.VMEM(state.shape, state.dtype),
        ),
        in_specs=[any_spec] * 16,
        out_specs=(vmem, vmem),
        scratch_shapes=[
            pltpu.VMEM((n, rows, width), BF16),
            pltpu.VMEM((1, width), F32),
            pltpu.VMEM((heads, 1, dim), F32),
            pltpu.VMEM((1, dim), F32),
            pltpu.VMEM((1, width), F32),
            pltpu.VMEM((4, width, cols), BF16),
            pltpu.VMEM((width, cols), BF16),
            pltpu.VMEM((width, hidden), BF16),
            pltpu.VMEM((width, hidden), BF16),
            pltpu.VMEM((hidden, width), BF16),
            pltpu.VMEM((total, width), BF16),
            pltpu.VMEM((n, rows, 4 * cols), BF16),
            pltpu.VMEM((n, rows, 4 * cols), BF16),
            pltpu.VMEM((heads, 4 * rows, dim), F32),
            pltpu.VMEM((n, rows, width), BF16),
            pltpu.VMEM((n, n // 2, 2 * rows, cols), BF16),
            pltpu.VMEM((n // 2, 2 * rows, width), F32),
            pltpu.VMEM((total, 1), F32),
            pltpu.VMEM((total, hidden), F32),
            pltpu.VMEM((total, hidden), F32),
            pltpu.VMEM((total, hidden), BF16),
            pltpu.VMEM((2, n // 2, rows, width), BF16),
            pltpu.VMEM((n // 2, rows, width), BF16),
            pltpu.VMEM((n // 2, rows, width), BF16),
            pltpu.VMEM((n // 2, rows, width), BF16),
            pltpu.VMEM(ids.T.shape, ids.dtype),
            pltpu.VMEM(weights.T.shape, weights.dtype),
            pltpu.SemaphoreType.DMA((16,)),
            pltpu.SemaphoreType.DMA((6,)),
            pltpu.SemaphoreType.DMA((3 * (n // 2) + 2,)),
            pltpu.SemaphoreType.REGULAR,
        ],
        compiler_params=pltpu.CompilerParams(
            collective_id=0,
            has_side_effects=True,
            vmem_limit_bytes=VMEM - 4 * state.size - 64 * 1024,
        ),
    )(
        tokens,
        state,
        ids.T,
        weights.T,
        norm_mix[None],
        w_query,
        w_forget,
        w_input,
        w_gate,
        lower_bound.reshape(heads, 1, dim),
        head_gain[None],
        w_out,
        norm_ffn[None],
        expert_gate,
        expert_up,
        expert_down,
    )
    return pl.pallas_call(
        write,
        out_shape=(
            jax.ShapeDtypeStruct(layer.shape, layer.dtype),
            jax.ShapeDtypeStruct(fresh.shape, fresh.dtype),
        ),
        in_specs=[vmem, vmem],
        out_specs=(any_spec, any_spec),
        scratch_shapes=[pltpu.SemaphoreType.DMA((1 + rows,))],
        compiler_params=pltpu.CompilerParams(vmem_limit_bytes=1 << 20),
    )(
        pltpu.with_memory_space_constraint(layer, pltpu.VMEM),
        pltpu.with_memory_space_constraint(fresh, pltpu.VMEM),
    )


def solution(mesh):
    return jax.shard_map(
        functools.partial(local, mesh.shape["ep"]),
        mesh=mesh,
        in_specs=(
            P(("grp", "ep"), None),
            P(("grp", "ep"), None, None, None),
            P(("grp", "ep"), None),
            P(("grp", "ep"), None),
            P(),
            P(None, "ep"),
            P(None, "ep"),
            P(None, "ep"),
            P(None, "ep"),
            P(),
            P(),
            P(None, "ep"),
            P(),
            P(None, "ep"),
            P(None, "ep"),
            P("ep", None),
        ),
        out_specs=(P(("grp", "ep"), None), P(("grp", "ep"), None, None, None)),
        check_vma=False,
    )
```

```python
import functools

import jax
import jax.numpy as jnp
from jax import lax
from jax.experimental import pallas as pl
from jax.experimental.pallas import tpu as pltpu
from jax.sharding import PartitionSpec as P

FF = 7168
EXPERTS = 4
VMEM = 67043328

epsilon = 1e-06
F32 = jnp.float32
BF16 = jnp.bfloat16


def rms_scale(values, gain):
    return values * lax.rsqrt(jnp.mean(values * values, axis=-1, keepdims=True) + epsilon) * gain


def kernel(
    n,
    tokens,
    state,
    ids_in,
    weights_in,
    norm_mix_in,
    w_query,
    w_forget,
    w_input,
    w_gate,
    lower_bound_in,
    head_gain_in,
    w_out,
    norm_ffn_in,
    expert_gate,
    expert_up,
    expert_down,
    layer_out,
    st,
    tok_buf,
    norm_mix,
    lower_bound,
    head_gain,
    norm_ffn,
    wp,
    wo,
    wg,
    wu,
    wd,
    xn,
    pj_send,
    pj_buf,
    gates,
    mx_buf,
    col_buf,
    mid_buf,
    squares,
    acc_gate,
    acc_up,
    hid,
    ps,
    fw,
    summed,
    ret_buf,
    ids,
    weights,
    load_sem,
    send_sem,
    recv_sem,
    late_sem,
):
    me = lax.axis_index("ep")
    rows, width = tokens.shape
    heads, dim = state.shape[1], state.shape[2]
    cols = w_query.shape[1]
    total = n * rows
    hidden = expert_gate.shape[1]
    group = n // EXPERTS // 2
    both = 2 * rows

    loads = [pltpu.make_async_copy(tokens, tok_buf.at[me], load_sem.at[0])]
    for j, w in enumerate((w_query, w_forget, w_input, w_gate)):
        loads.append(pltpu.make_async_copy(w, wp.at[j], load_sem.at[1 + j]))
    loads.append(pltpu.make_async_copy(state, st, load_sem.at[5]))
    loads.append(pltpu.make_async_copy(w_out, wo, load_sem.at[6]))
    loads.append(pltpu.make_async_copy(expert_gate, wg, load_sem.at[7]))
    loads.append(pltpu.make_async_copy(expert_up, wu, load_sem.at[8]))
    loads.append(pltpu.make_async_copy(expert_down, wd, load_sem.at[9]))
    loads.append(pltpu.make_async_copy(ids_in, ids, load_sem.at[14]))
    loads.append(pltpu.make_async_copy(weights_in, weights, load_sem.at[15]))
    small = [
        pltpu.make_async_copy(a, b, load_sem.at[10 + j])
        for j, (a, b) in enumerate(
            (
                (norm_mix_in, norm_mix),
                (lower_bound_in, lower_bound),
                (head_gain_in, head_gain),
                (norm_ffn_in, norm_ffn),
            )
        )
    ]

    core = lax.rem(me, 2)
    chip = me // 2
    chips = n // 2
    partner = me + 1 - 2 * core

    def flip(index, k):
        bit = 1
        while bit <= k:
            if k & bit:
                index = index + bit * (1 - 2 * lax.rem(index // bit, 2))
            bit *= 2
        return index

    bits = [1 << b for b in range(chips.bit_length() - 1)]
    at = [flip(chip, k) for k in range(chips)]
    same = [2 * at[k] + core for k in range(chips)]
    cross = [2 * at[k] + 1 - core for k in range(chips)]
    far_first = list(range(chips - 1, 0, -1))
    barrier = pltpu.get_barrier_semaphore()
    late = chip == chips - 1

    def signal(semaphore, peer):
        pl.semaphore_signal(
            semaphore, inc=1, device_id={"ep": peer}, device_id_type=pl.DeviceIdType.MESH
        )

    @pl.when(late)
    def _():
        signal(barrier, partner)

    @pl.when(jnp.logical_not(late))
    def _():
        for k in far_first:
            signal(barrier, same[k])
            signal(barrier, cross[k])
        signal(barrier, partner)

    loads[0].start()

    @pl.when(late)
    def _():
        pl.semaphore_wait(barrier, n - 1)
        for k in far_first:
            signal(late_sem, same[k])
            signal(late_sem, cross[k])

    for load in small + loads[1:]:
        load.start()

    @pl.when(jnp.logical_not(late))
    def _():
        pl.semaphore_wait(barrier, n - 3)

    GATHER, MOVE, MIXED, COLUMNS, PAIR, RETURN = range(6)

    second, third = chips + chips // 2, 2 * chips + 1

    def lane(phase, slot, direct):
        if phase == MOVE:
            return second + slot // 4
        if phase == PAIR or (phase == MIXED and direct and slot):
            return third + slot
        if phase == RETURN:
            return third + chips
        if phase == COLUMNS and not direct:
            if slot == chips + 1:
                return second + chips // 2
            return second + (slot - chips) // 2 if slot else second
        return slot if direct else chips + (slot - chips) // 2

    def handle(phase, slot, source, target, peer, direct=False):
        return pltpu.make_async_remote_copy(
            src_ref=source,
            dst_ref=target,
            send_sem=send_sem.at[phase],
            recv_sem=recv_sem.at[lane(phase, slot, direct)],
            device_id={"ep": peer},
            device_id_type=pl.DeviceIdType.MESH,
        )

    def send(phase, slot, source, target, peer, direct=False):
        copy = handle(phase, slot, source, target, peer, direct)
        copy.start()
        return copy

    def whole(phase, slot, block, direct=False):
        return handle(phase, slot, block, block, partner, direct)

    def scatter(phase, block, near=0):
        for k in far_first:
            send(phase, k, block, block, cross[k], True)
            if k <= near:
                send(phase, chips + k, block, block, same[k])

    def forward(phase, buf, ks, near=0):
        for k in ks:
            if k == 0:
                send(phase, 0, buf.at[me], buf.at[me], partner, phase != COLUMNS)
            else:
                block = buf.at[cross[k]]
                whole(phase, k, block, True).wait_recv()
                if k > near:
                    send(phase, chips + k, block, block, partner)
                else:
                    whole(phase, chips + k, buf.at[same[k]]).wait_recv()

    def arrive(phase, buf, ks, near=0):
        for k in ks[::2]:
            if k:
                whole(phase, chips + k, buf.at[pl.ds(0, 2)]).wait_recv()
            else:
                whole(phase, 0, buf.at[0], phase != COLUMNS).wait_recv()
                if near < 1:
                    whole(phase, chips + 1, buf.at[0]).wait_recv()

    shares = [(chips * i // 4, chips * (i + 1) // 4) for i in range(4)]

    def base_of(index, lo, hi):
        return flip(index // (hi - lo), lo // (hi - lo)) * (hi - lo)

    def chip_rows(buf, k):
        return [buf[2 * at[k] + c].astype(F32) for c in range(2)]
    loads[0].wait()
    own = tok_buf.at[me]
    to_late = sum(bit * (1 - lax.rem(chip // bit, 2)) for bit in bits)
    direct = [handle(GATHER, k, own, own, cross[k] if k else partner, True) for k in range(chips)]
    extra = pltpu.make_async_remote_copy(
        src_ref=own,
        dst_ref=own,
        send_sem=send_sem.at[GATHER],
        recv_sem=recv_sem.at[chips + to_late // 2],
        device_id={"ep": n - 2 + core},
        device_id_type=pl.DeviceIdType.MESH,
    )
    for k in far_first:

        @pl.when(at[k] != chips - 1)
        def _(k=k):
            direct[k].start()

    @pl.when(jnp.logical_not(late))
    def _():
        direct[0].start()
        pl.semaphore_wait(late_sem, 2)
        extra.start()

    handle(GATHER, to_late, own, own, n - 1 - core, True).start()

    for load in small:
        load.wait()
    pairs = [[2 * j, 2 * j + 1] for j in range(chips // 2)]

    def norm_pair(j):
        x = jnp.concatenate([tok_buf[4 * j + i].astype(F32) for i in range(4)], axis=0)
        for i in range(2):
            mid_buf[2 * j + i] = x[i * both : (i + 1) * both, :]
        span = pl.ds(pl.multiple_of(2 * j * both, 2 * both), 2 * both)
        xn[span, :] = rms_scale(x, norm_mix[...]).astype(BF16)

    def relation(index):
        return sum(bit * lax.rem(chip // bit + index // bit, 2) for bit in bits)

    def pass_on(index):
        slot = relation(index)
        whole(GATHER, slot, own, True).wait_recv()

        @pl.when(jnp.logical_not(late))
        def _():
            block = tok_buf.at[2 * index + 1 - core]
            send(GATHER, chips + slot, block, block, partner)

    def settle_pair(j, first):
        if first:
            whole(GATHER, chips + 1, own).wait_recv()
        else:
            whole(GATHER, chips + relation(2 * j), tok_buf.at[pl.ds(0, 2)]).wait_recv()
        norm_pair(j)

    plane, planes = chip // 2, chips // 2
    order = [plane]
    for i in range(planes - 1):
        above = (i < planes - 1 - plane).astype(jnp.int32)
        order.append(above * (plane + 1 + i) + (1 - above) * (planes - 2 - i))
    whole(GATHER, 0, own, True).wait_recv()
    pass_on(at[1])
    for i in range(1, planes):
        pass_on(2 * order[i])
        pass_on(2 * order[i] + 1)
        settle_pair(order[i - 1], i == 1)
    settle_pair(order[-1], planes == 1)
    for load in loads[1:5]:
        load.wait()
    w_all = jnp.concatenate([wp[j] for j in range(4)], axis=1)
    acc = jnp.dot(xn[...], w_all, preferred_element_type=F32)
    for s in range(n):
        pj_send[s] = acc[s * rows : (s + 1) * rows, :].astype(BF16)
    for k in far_first + [0]:
        for r, peer in enumerate((same[k], cross[k])):
            if k or r:
                send(MOVE, 2 * k + r, pj_send.at[peer], pj_buf.at[me], peer)
    pj_buf[me] = pj_send[me]
    per_head = max(1, dim // cols)
    head_chips = max(1, per_head // 2)
    chip_heads = head_chips * 2 * cols // dim
    loads[5].wait()

    def head_step(h, first):
        def owned(j):
            return jnp.concatenate(
                [
                    pj_buf[first + i][:, j * cols : (j + 1) * cols].astype(F32)
                    for i in range(per_head)
                ],
                axis=1,
            )

        bound = lower_bound[h]
        forget_raw = owned(1)
        decay = bound + (1.0 - bound) * jax.nn.sigmoid(forget_raw)
        key_vec = (1.0 - bound) * jax.nn.sigmoid(-forget_raw)
        query_vec = jax.nn.silu(owned(0)) * dim ** (-0.5)
        input_raw = owned(2)
        read_vec = query_vec * decay
        gates[h] = jnp.concatenate([read_vec, decay, key_vec, input_raw], axis=0)
        wide = jnp.dot(
            read_vec,
            jnp.concatenate([st[t, h] for t in range(rows)], axis=1),
            preferred_element_type=F32,
        )
        read = jnp.concatenate(
            [wide[t : t + 1, t * dim : (t + 1) * dim] for t in range(rows)], axis=0
        ) + input_raw * jnp.sum(query_vec * key_vec, axis=1, keepdims=True)
        mixed = rms_scale(read, head_gain[...]) * jax.nn.silu(owned(3))
        part = pl.ds(pl.multiple_of(h * dim, dim), dim)
        mx_buf[me, :, part] = mixed.astype(BF16)

    for lo, hi in shares:
        step = max(2, head_chips)
        for first in range(lo, hi, step):
            for k in range(first, first + step, 2):
                count = 4 if k else 3
                whole(MOVE, 2 * k, pj_buf.at[pl.ds(0, count)]).wait_recv()
            for m in range(first // head_chips, (first + step) // head_chips):
                base = flip(chip // head_chips, m)
                for i in range(chip_heads):
                    head_step(base * chip_heads + i, base * head_chips * 2 + i * per_head)
        size = (hi - lo) * 2 * cols
        offset = pl.multiple_of(base_of(chip, lo, hi) * 2 * cols, size)
        scatter(MIXED, mx_buf.at[me, :, pl.ds(offset, size)])

    def update_step(h, carry):
        flat = gates[h]
        turned = flat.T
        for t in range(rows):
            st[t, h] = (
                turned[:, rows + t : rows + t + 1] * st[t, h]
                + turned[:, 2 * rows + t : 2 * rows + t + 1]
                * flat[3 * rows + t : 3 * rows + t + 1, :]
            )
        return carry

    cuts = [heads * c // 16 for c in (0, 8, 11, 13, 16)]

    def update(c):
        lax.fori_loop(cuts[c], cuts[c + 1], update_step, 0, unroll=2)
    forward(MIXED, mx_buf, [0])
    loads[6].wait()
    update(0)
    near = min(1, chips - 1)

    def gather_pair(ks):
        arrive(MIXED, mx_buf, ks)
        x = jnp.concatenate([part for k in ks for part in chip_rows(mx_buf, k)], axis=0)
        xn[ks[0] * both : (ks[0] + 2) * both, :] = x.astype(BF16)

    def project(lo, hi):
        acc = jnp.dot(xn[lo * both : hi * both, :], wo[...], preferred_element_type=F32)
        for k in range(lo, hi):
            col_buf[me, at[k]] = acc[(k - lo) * both : (k - lo + 1) * both, :].astype(BF16)
        base = base_of(chip, lo, hi)
        scatter(COLUMNS, col_buf.at[me, pl.ds(base, hi - lo)], near)

    for j, ks in enumerate(pairs):
        forward(MIXED, mx_buf, [k for k in ks if k])
        if j:
            gather_pair(pairs[j - 1])
            ready = 2 * j
            if ready == chips // 4:
                project(0, ready)
            if ready == chips // 2:
                project(chips // 4, ready)
    gather_pair(pairs[-1])
    project(chips // 2, chips)
    forward(COLUMNS, col_buf, [0])
    update(1)
    loads[7].wait()
    loads[8].wait()
    tile = 256 if hidden % 256 == 0 else hidden
    slab_chips = max(1, 256 // (2 * cols))
    slab = slab_chips * 2 * cols
    slabs = chips // slab_chips

    def piece_of(first, count, offset, size):
        part = pl.ds(pl.multiple_of(offset, size), size)
        y = jnp.concatenate([col_buf[first + i].astype(F32) for i in range(count)], axis=2)
        middle = mid_buf[:, :, part] + y
        mid_buf[:, :, part] = middle
        scaled = (middle * norm_ffn[:, part]).reshape(total, size).astype(BF16)
        return part, scaled, jnp.sum((middle * middle).reshape(total, size), axis=1, keepdims=True)

    steps = []
    if cols % 128 == 0:

        def devices(peers):
            return [(peer, 1, peer * cols, cols) for peer in peers]

        steps.append(([], [0], [(2 * chip, 2, chip * slab, slab)]))
        if near:
            steps.append(([1], [], [(2 * at[1], 2, at[1] * slab, slab)]))
        rest = [[k, k + 1] for k in range(2 * near, chips, 2)]
        for ks in rest:
            steps.append((ks, [], devices(cross[k] for k in ks)))
        for ks in rest:
            steps.append(([], ks, devices(same[k] for k in ks)))
    else:
        for m in range(slabs):
            ks = list(range(m * slab_chips, (m + 1) * slab_chips))
            base = flip(chip // slab_chips, m)
            steps.append((ks[m == 0 :], ks, [(base * slab_chips * 2, 2 * slab_chips, base * slab, slab)]))

    for m, (coming, there, pieces) in enumerate(steps):
        forward(COLUMNS, col_buf, coming, near)
        arrive(COLUMNS, col_buf, there, near)
        ready = [piece_of(*piece) for piece in pieces]
        power = sum(piece[2] for piece in ready)
        scaled = jnp.concatenate([piece[1] for piece in ready], axis=1)
        if m:
            power = power + squares[...]
        last = m + 1 == len(steps)
        if last:
            scale = lax.rsqrt(power / width + epsilon)
        else:
            squares[...] = power
        for j in range(hidden // tile):
            span = slice(j * tile, (j + 1) * tile)
            g_rows = jnp.concatenate([wg[piece[0], span] for piece in ready], axis=0)
            u_rows = jnp.concatenate([wu[piece[0], span] for piece in ready], axis=0)
            g = jnp.dot(scaled, g_rows, preferred_element_type=F32)
            u = jnp.dot(scaled, u_rows, preferred_element_type=F32)
            if m:
                g = g + acc_gate[:, span]
                u = u + acc_up[:, span]
            if last:
                hid[:, span] = (jax.nn.silu(g * scale) * (u * scale)).astype(BF16)
            else:
                acc_gate[:, span] = g
                acc_up[:, span] = u
        if m == 0:
            update(2)
    loads[9].wait()
    out_tile = 256
    counts = [1] + [2] * (width // (2 * out_tile) - 2) + [3]
    bounds = [sum(counts[:p]) * out_tile for p in range(len(counts) + 1)]

    halves = []

    def settle(p):
        part = pl.ds(bounds[p], bounds[p + 1] - bounds[p])
        halves[p].wait_recv()
        for c in range(chips):
            summed[c, :, part] = (
                ps[1 - core, c, :, part].astype(F32) + fw[c, :, part].astype(F32)
            ).astype(BF16)
        for k in far_first + [0]:
            send(
                RETURN, k, summed.at[at[k], :, part], ret_buf.at[chip, :, part], cross[k]
            )

    for p in range(len(counts)):
        for q in range(counts[p]):
            part = slice(bounds[p] + q * out_tile, bounds[p] + (q + 1) * out_tile)
            d = jnp.dot(hid[...], wd[:, part], preferred_element_type=F32)
            for s in range(n):
                ps[s % 2, s // 2, :, part] = d[s * rows : (s + 1) * rows, :].astype(BF16)
        part = pl.ds(bounds[p], bounds[p + 1] - bounds[p])
        halves.append(send(PAIR, p, ps.at[core, :, :, part], fw.at[:, :, part], partner))
        if p >= 2:
            settle(p - 2)
    for p in range(len(counts) - 2, len(counts)):
        settle(p)
    update(3)
    for phase, buf in ((MOVE, pj_send), (MIXED, mx_buf), (COLUMNS, col_buf)):
        whole(phase, 0, buf.at[pl.ds(0, n - 1)]).wait_send()
    whole(PAIR, 0, ps.at[0]).wait_send()

    @pl.when(late)
    def _():
        whole(GATHER, 0, tok_buf.at[pl.ds(0, chips)]).wait_send()

    @pl.when(jnp.logical_not(late))
    def _():
        whole(GATHER, 0, tok_buf).wait_send()
    whole(RETURN, 0, ret_buf).wait_recv()
    for load in loads[10:]:
        load.wait()
    own = mid_buf[chip]
    result = jnp.where(core == 0, own[:rows, :], own[rows:, :])
    diagonal = lax.broadcasted_iota(jnp.int32, (rows, rows), 0) == lax.broadcasted_iota(
        jnp.int32, (rows, rows), 1
    )
    for e in range(EXPERTS):
        flat_share = jnp.sum(
            jnp.where(ids[...] == e, weights[...].astype(F32), 0.0), axis=0, keepdims=True
        )
        share = jnp.sum(jnp.where(diagonal, flat_share, 0.0), axis=1, keepdims=True)
        rows_e = ret_buf[e * group].astype(F32)
        for s in range(1, group):
            rows_e = rows_e + ret_buf[e * group + s].astype(F32)
        result = result + share * rows_e
    layer_out[...] = result.astype(BF16)
    whole(RETURN, 0, summed).wait_send()


def write(layer_in, state_in, layer_out, state_out, sem):
    copies = [pltpu.make_async_copy(layer_in, layer_out, sem.at[0])]
    for t in range(state_in.shape[0]):
        copies.append(pltpu.make_async_copy(state_in.at[t], state_out.at[t], sem.at[1 + t]))
    for copy in copies:
        copy.start()
    for copy in copies:
        copy.wait()


def local(n, *args):
    (
        tokens,
        state,
        ids,
        weights,
        norm_mix,
        w_query,
        w_forget,
        w_input,
        w_gate,
        lower_bound,
        head_gain,
        w_out,
        norm_ffn,
        expert_gate,
        expert_up,
        expert_down,
    ) = args
    rows, width = tokens.shape
    heads, dim = state.shape[1], state.shape[2]
    cols = w_query.shape[1]
    hidden = expert_gate.shape[1]
    total = n * rows
    any_spec = pl.BlockSpec(memory_space=pltpu.HBM)
    vmem = pl.BlockSpec(memory_space=pltpu.VMEM)
    layer, fresh = pl.pallas_call(
        functools.partial(kernel, n),
        out_shape=(
            pltpu.VMEM(tokens.shape, tokens.dtype),
            pltpu.VMEM(state.shape, state.dtype),
        ),
        in_specs=[any_spec] * 16,
        out_specs=(vmem, vmem),
        scratch_shapes=[
            pltpu.VMEM((n, rows, width), BF16),
            pltpu.VMEM((1, width), F32),
            pltpu.VMEM((heads, 1, dim), F32),
            pltpu.VMEM((1, dim), F32),
            pltpu.VMEM((1, width), F32),
            pltpu.VMEM((4, width, cols), BF16),
            pltpu.VMEM((width, cols), BF16),
            pltpu.VMEM((width, hidden), BF16),
            pltpu.VMEM((width, hidden), BF16),
            pltpu.VMEM((hidden, width), BF16),
            pltpu.VMEM((total, width), BF16),
            pltpu.VMEM((n, rows, 4 * cols), BF16),
            pltpu.VMEM((n, rows, 4 * cols), BF16),
            pltpu.VMEM((heads, 4 * rows, dim), F32),
            pltpu.VMEM((n, rows, width), BF16),
            pltpu.VMEM((n, n // 2, 2 * rows, cols), BF16),
            pltpu.VMEM((n // 2, 2 * rows, width), F32),
            pltpu.VMEM((total, 1), F32),
            pltpu.VMEM((total, hidden), F32),
            pltpu.VMEM((total, hidden), F32),
            pltpu.VMEM((total, hidden), BF16),
            pltpu.VMEM((2, n // 2, rows, width), BF16),
            pltpu.VMEM((n // 2, rows, width), BF16),
            pltpu.VMEM((n // 2, rows, width), BF16),
            pltpu.VMEM((n // 2, rows, width), BF16),
            pltpu.VMEM(ids.T.shape, ids.dtype),
            pltpu.VMEM(weights.T.shape, weights.dtype),
            pltpu.SemaphoreType.DMA((16,)),
            pltpu.SemaphoreType.DMA((6,)),
            pltpu.SemaphoreType.DMA((3 * (n // 2) + 2,)),
            pltpu.SemaphoreType.REGULAR,
        ],
        compiler_params=pltpu.CompilerParams(
            collective_id=0,
            has_side_effects=True,
            vmem_limit_bytes=VMEM - 4 * state.size - 64 * 1024,
        ),
    )(
        tokens,
        state,
        ids.T,
        weights.T,
        norm_mix[None],
        w_query,
        w_forget,
        w_input,
        w_gate,
        lower_bound.reshape(heads, 1, dim),
        head_gain[None],
        w_out,
        norm_ffn[None],
        expert_gate,
        expert_up,
        expert_down,
    )
    return pl.pallas_call(
        write,
        out_shape=(
            jax.ShapeDtypeStruct(layer.shape, layer.dtype),
            jax.ShapeDtypeStruct(fresh.shape, fresh.dtype),
        ),
        in_specs=[vmem, vmem],
        out_specs=(any_spec, any_spec),
        scratch_shapes=[pltpu.SemaphoreType.DMA((1 + rows,))],
        compiler_params=pltpu.CompilerParams(vmem_limit_bytes=1 << 20),
    )(
        pltpu.with_memory_space_constraint(layer, pltpu.VMEM),
        pltpu.with_memory_space_constraint(fresh, pltpu.VMEM),
    )


def solution(mesh):
    return jax.shard_map(
        functools.partial(local, mesh.shape["ep"]),
        mesh=mesh,
        in_specs=(
            P(("grp", "ep"), None),
            P(("grp", "ep"), None, None, None),
            P(("grp", "ep"), None),
            P(("grp", "ep"), None),
            P(),
            P(None, "ep"),
            P(None, "ep"),
            P(None, "ep"),
            P(None, "ep"),
            P(),
            P(),
            P(None, "ep"),
            P(),
            P(None, "ep"),
            P(None, "ep"),
            P("ep", None),
        ),
        out_specs=(P(("grp", "ep"), None), P(("grp", "ep"), None, None, None)),
        check_vma=False,
    )
```
